512 devices in a mesh: sp: 32 (over z, core), tp: 16 (over y, x).
Axes of the slice: x: 4, y: 4, z: 16, core: 2. Of those that a mesh axis runs over, the one named last changes fastest.
Arguments:
- layer_input: bfloat16 [8, 4096, 2048], P(None, 'sp', 'tp'), may hold values from -6 to 6
- w_key: bfloat16 [2048, 2048], P(None, 'tp'), may hold values from -0.125 to 0.125
- w_value: bfloat16 [2048, 2048], P(None, 'tp'), may hold values from -0.125 to 0.125
- w_gates: bfloat16 [2, 2048, 16], replicated, may hold values from -0.125 to 0.125
- decay_rate: float32 [16], P('tp'), may hold values from 0 to 1, as said below
- beta_bias: float32 [16], P('tp'), may hold values from -5.5 to -3
- log_decay_extra: float32 [8, 16, 4096], P(None, 'tp', 'sp'), may hold values from -2 to 0, as said below
- new_query: bfloat16 [8, 2048], P(None, 'tp'), may hold values from -6 to 6
- read_gain: float32 [128], replicated, may hold values from 0.1 to 1.9
Outputs:
- state_cache: bfloat16 [1024, 2048], P('sp', 'tp')
- first_read: bfloat16 [8, 2048], P(None, 'tp')
The draws below stay inside these ranges and needn't reach their ends.
Inputs may be any that keep to these rules, and one draw needn't show every extreme that they name: `decay_rate`: a positive rate for each head. `log_decay_extra`: additions that are never positive.
All inputs are finite; a program needn't handle non-finite values.
Results may differ from the reference program's by a relative error of at most 0.0052.
Values may be sent and summed in bfloat16 or wider, within the bound.
No kernel may reach another device: no remote copies, remote signals or barrier semaphores. Data moves between devices by JAX's collectives and lax.ppermute only.
A program may use at most 64 MiB of HBM per device.

```python
import math
import jax
import jax.numpy as jnp
from jax import lax

D = 2048
H = 16
DK = 128
DV = 128
BLOCK = 64
SEQS = 8
SEG = 128
LEN = 4096


def draw_decay_rate(key, part):
    pick_key, fast_key, slow_key = jax.random.split(jax.random.fold_in(key, 11), 3)
    share = 0.5
    coin = jax.random.uniform(pick_key, (H,), jnp.float32)
    fast = jnp.exp(jax.random.uniform(fast_key, (H,), jnp.float32, math.log(0.04), math.log(0.1)))
    slow = jnp.exp(jax.random.uniform(slow_key, (H,), jnp.float32, math.log(0.05), math.log(0.3))) / LEN
    return jnp.where(coin < share, fast, slow).astype(jnp.float32)


def draw_log_decay_extra(key, part):
    block_key, place_key, depth_key = jax.random.split(jax.random.fold_in(key, 23), 3)
    factor = jnp.exp(jax.random.uniform(block_key, (SEQS, LEN // SEG), jnp.float32, math.log(0.1), math.log(1.0)))
    starting_shift = -jnp.repeat(factor, SEG, axis=1) / LEN
    stored_slots = jax.random.randint(place_key, (SEQS, 2), 0, LEN)
    stack_levels = jax.random.uniform(depth_key, (SEQS, 2), jnp.float32, math.log(0.5), math.log(0.8))
    sequence_indices = jnp.arange(LEN)
    emitted_span = jnp.sum(jnp.where(sequence_indices[None, None, :] == stored_slots[:, :, None], stack_levels[:, :, None], 0.0), axis=1)
    overall_count = starting_shift + emitted_span
    return jnp.broadcast_to(overall_count[:, None, :], (SEQS, H, LEN)).astype(jnp.float32)


def level_of(stream_key, dims, cuts, low, top_value):
    level = 1.0
    for axis_at, blocks in cuts:
        steps = jax.random.uniform(jax.random.fold_in(jax.random.fold_in(stream_key, 6), axis_at), (blocks,), jnp.float32, low / len(cuts), top_value / len(cuts))
        level = level * jnp.repeat(jnp.exp(steps), dims[axis_at] // blocks).reshape((-1,) + (1,) * (len(dims) - 1 - axis_at))
    return level


def noise(key, shape, scale, reach, cuts=(), kind=jnp.bfloat16):
    values = jax.random.normal(key, shape, jnp.float32) * scale
    if len(cuts) > 0:
        values = level_of(key, shape, cuts, -0.22, 0.18) * values
    return jnp.clip(values, min=-reach, max=reach).astype(kind)


def setup_inputs(seed: int = 0) -> dict:
    key_of = jax.random.split(jax.random.key(seed), 10)
    return {
        "layer_input": noise(key_of[0], (SEQS, LEN, D), 1.0, 6.0, ((1, 32), (2, 16))),
        "w_key": noise(key_of[1], (D, H * DK), D ** -0.5, 0.125, ((1, 16),)),
        "w_value": noise(key_of[2], (D, H * DV), D ** -0.5, 0.125, ((1, 16),)),
        "w_gates": noise(key_of[3], (2, D, H), D ** -0.5, 0.125),
        "decay_rate": draw_decay_rate(jax.random.fold_in(key_of[9], 71), 0),
        "beta_bias": jnp.clip(-5.5 + 2.5 * jax.random.uniform(key_of[5], (H,), jnp.float32) ** level_of(key_of[5], (H,), ((0, 16),), -0.2, 0.2), -5.5, -3.0),
        "log_decay_extra": draw_log_decay_extra(jax.random.fold_in(key_of[9], 71), 0),
        "new_query": noise(key_of[7], (SEQS, H * DK), 1.0, 6.0, ((1, 16),)),
        "read_gain": jnp.clip(1.0 + 0.18 * jax.random.normal(key_of[8], (DV,), jnp.float32), 0.1, 1.9),
    }


EPS = 1e-06
HIGH = lax.Precision.HIGHEST

def unit_rows(values):
    return values * lax.rsqrt(lax.optimization_barrier(jnp.sum(values * values, axis=-1, keepdims=True)) + EPS)

def block_pieces(keys, values, log_decay, beta):
    size = keys.shape[-2]
    width = values.shape[-1]
    running = jnp.cumsum(log_decay, axis=-1)
    sequence_indices = jnp.arange(size)
    causal = sequence_indices[:, None] >= sequence_indices[None, :]
    strict = sequence_indices[:, None] > sequence_indices[None, :]
    spread = running[..., :, None] - running[..., None, :]
    weights = jnp.where(causal, jnp.exp(jnp.where(causal, spread, 0.0)), 0.0)
    key_beta = keys * beta[..., None]
    lower = jnp.where(strict, jnp.einsum('...cd,...sd->...cs', key_beta, keys, precision=HIGH) * weights, 0.0)
    right_side = jnp.concatenate([values * beta[..., None], key_beta * jnp.exp(running)[..., None]], axis=-1)
    solved = lax.linalg.triangular_solve(lower, right_side, left_side=True, lower=True, unit_diagonal=True)
    fresh = solved[..., :width]
    erase = solved[..., width:]
    last = running[..., -1]
    key_late = keys * jnp.exp(last[..., None] - running)[..., None]
    identity = jnp.eye(keys.shape[-1], dtype=jnp.float32)
    transition = jnp.exp(last)[..., None, None] * identity - jnp.einsum('...cd,...ce->...de', key_late, erase, precision=HIGH)
    inject = jnp.einsum('...cd,...cv->...dv', key_late, fresh, precision=HIGH)
    return (transition, inject)

def reference(layer_input, w_key, w_value, w_gates, decay_rate, beta_bias, log_decay_extra, new_query, read_gain):
    blocks = LEN // BLOCK

    def one_prompt(pair):
        rows, extra = pair
        key_pre = jnp.dot(rows.astype(jnp.float32), w_key.astype(jnp.float32), preferred_element_type=jnp.float32).reshape(LEN, H, DK)
        value_pre = jnp.dot(rows.astype(jnp.float32), w_value.astype(jnp.float32), preferred_element_type=jnp.float32).reshape(LEN, H, DV)
        decay_pre = jnp.dot(rows.astype(jnp.float32), w_gates[0].astype(jnp.float32), preferred_element_type=jnp.float32)
        beta_pre = jnp.dot(rows.astype(jnp.float32), w_gates[1].astype(jnp.float32), preferred_element_type=jnp.float32)
        keys = unit_rows(jax.nn.silu(key_pre))
        values = jax.nn.silu(value_pre)
        log_decay = -decay_rate[None, :] * jax.nn.softplus(decay_pre) + extra.T
        beta = jax.nn.sigmoid(beta_pre + beta_bias[None, :])
        key_blocks = keys.reshape(blocks, BLOCK, H, DK).transpose(2, 0, 1, 3)
        value_tiles = values.reshape(blocks, BLOCK, H, DV).transpose(2, 0, 1, 3)
        decay_blocks = log_decay.reshape(blocks, BLOCK, H).transpose(2, 0, 1)
        strength_groups = beta.reshape(blocks, BLOCK, H).transpose(2, 0, 1)
        transition, inject = block_pieces(key_blocks, value_tiles, decay_blocks, strength_groups)

        def advance(state, piece):
            block_map, block_add = piece
            return (jnp.einsum('hde,hev->hdv', block_map, state, precision=HIGH) + block_add, None)
        start = jnp.zeros((H, DK, DV), jnp.float32)
        state, _ = lax.scan(advance, start, (jnp.moveaxis(transition, 1, 0), jnp.moveaxis(inject, 1, 0)))
        return state
    final_state = lax.map(one_prompt, (layer_input, log_decay_extra))
    cached = final_state.astype(jnp.bfloat16)
    state_cache = cached.transpose(0, 2, 1, 3).reshape(SEQS * DK, H * DV)
    query = new_query.reshape(SEQS, H, DK).astype(jnp.float32)
    raw_read = jnp.einsum('shav,sha->shv', cached.astype(jnp.float32), query, precision=HIGH)
    scaled = raw_read * lax.rsqrt(lax.optimization_barrier(jnp.mean(raw_read * raw_read, axis=-1, keepdims=True)) + EPS) * read_gain
    first_read = scaled.astype(jnp.bfloat16).reshape(SEQS, H * DV)
    return (state_cache, first_read)
```

```python
import jax
import jax.numpy as jnp
from jax import lax
from jax.experimental import pallas as pl
from jax.experimental.pallas import tpu as pltpu
from jax.sharding import PartitionSpec as P


DK = 128
DV = 128
BLOCK = 128
EPS = 1e-06
HIGH = lax.Precision.HIGHEST
F32 = jnp.float32
BF16 = jnp.bfloat16
PAD = 16


MIB = 1 << 20
VMEM = pl.BlockSpec(memory_space=pltpu.VMEM)
SMEM = pl.BlockSpec(memory_space=pltpu.SMEM)


def granted(mib):
    return pltpu.CompilerParams(vmem_limit_bytes=mib * MIB)


NN = (((1,), (0,)), ((), ()))
NT = (((1,), (1,)), ((), ()))


def dot1(left, right, dims=NN):
    return lax.dot_general(left, right, dims, preferred_element_type=F32)


def halves(x):
    high = x.astype(BF16)
    low = (x - high.astype(F32)).astype(BF16)
    return high, low


def dot3(left, right, dims=NN):
    lh, ll = left if isinstance(left, tuple) else halves(left)
    rh, rl = right if isinstance(right, tuple) else halves(right)
    return dot1(lh, rh, dims) + (dot1(ll, rh, dims) + dot1(lh, rl, dims))


def unit_lower_inverse(low, row, col):
    size = low.shape[0]
    eye = (row == col).astype(F32)
    step = 1
    inverse = eye
    while step < size:
        merge = ((row // (2 * step)) == (col // (2 * step))) & ((row // step) != (col // step))
        part = jnp.where(merge, low, 0.0)
        if step == 1:
            inverse = eye - part
        else:
            held = inverse.astype(BF16)
            inverse = inverse - dot1(dot1(held, part.astype(BF16)).astype(BF16), held)
        step *= 2
    return inverse


def three_pieces(x):
    high = x.astype(BF16).astype(F32)
    rest = x - high
    mid = rest.astype(BF16).astype(F32)
    return high, mid, (rest - mid).astype(BF16).astype(F32)


def pack_kernel(x, extra, out):
    prompts, seg, width = x.shape
    out[:, :seg, :] = x[...]
    pieces = three_pieces(extra[...])
    for p in range(prompts):
        rows = [piece[p : p + 1] for piece in pieces] + [jnp.zeros((PAD - 3, width), F32)]
        out[p, seg:, :] = jnp.concatenate(rows, axis=0).astype(BF16)


def packed(layer_input, extra):
    prompts, seg, width = layer_input.shape
    return pl.pallas_call(
        pack_kernel,
        in_specs=[VMEM, VMEM],
        out_specs=VMEM,
        out_shape=jax.ShapeDtypeStruct((prompts, seg + PAD, width), BF16),
        compiler_params=granted(4),
    )(layer_input, extra)


def parcel_kernel(here, rate, bias, out):
    segs, rows, width = here.shape
    seg = rows - PAD
    half = segs // 2
    lane = lax.broadcasted_iota(jnp.int32, (1, width), 1)
    consts = three_pieces(jnp.where(lane < width // 2, rate[0], bias[0]))
    for which in range(2):
        tails = [here[half * which + b, seg:, :].astype(F32) for b in range(half)]
        tail = [tails[b][i : i + 1] for i in range(3) for b in range(half)]
        tail = jnp.concatenate(tail + list(consts) + [jnp.zeros((PAD - 3 * half - 3, width), F32)], axis=0)
        tail = tail.astype(BF16)
        body = [here[half * which + b, :seg, :] for b in range(half)]
        for other in range(which, out.shape[0], 2):
            for b in range(half):
                out[other, seg * b : seg * (b + 1), :] = body[b]
            out[other, seg * half :, :] = tail


def parcels(here, rate, bias, count):
    segs, rows, width = here.shape
    return pl.pallas_call(
        parcel_kernel,
        in_specs=[VMEM, SMEM, SMEM],
        out_specs=VMEM,
        out_shape=jax.ShapeDtypeStruct((count, (segs // 2) * (rows - PAD) + PAD, width), BF16),
        compiler_params=granted(8),
    )(here, rate, bias)


def map_kernel(xg, wk, wv, wo, wg, mine, other, acc, gates):
    sources, rows, width = xg.shape
    rows = rows - PAD
    blocks = rows // BLOCK
    me = lax.axis_index("tp")
    x = jnp.concatenate([xg[i, :rows, :] for i in range(sources)], axis=1)
    acc[0] = dot1(x, jnp.concatenate([wk[...], wv[...]], axis=1))
    acc[1] = dot1(x, jnp.concatenate([wo[0], wo[1]], axis=1))
    gates[...] = dot1(wg[...], x, NT)

    row = lax.broadcasted_iota(jnp.int32, (BLOCK, BLOCK), 0)
    col = lax.broadcasted_iota(jnp.int32, (BLOCK, BLOCK), 1)
    upto = (row <= col).astype(F32)
    decays, betas = [], []
    for which in range(2):
        head = me if which == 0 else me ^ 1
        extras = xg[head, rows:, :].astype(F32)
        extra = extras[0:4] + extras[4:8] + extras[8:12]
        consts = extras[12:13] + extras[13:14] + extras[14:15]
        rate, bias = consts[:, 0:1], consts[:, width // 2 : width // 2 + 1]
        cut = lambda g: jnp.concatenate(
            [g[:, BLOCK * b : BLOCK * (b + 1)] for b in range(blocks)], axis=0
        )
        decay_pre = cut(gates[pl.ds(head, 1), :])
        beta_pre = cut(gates[pl.ds(sources + head, 1), :])
        soft = jnp.maximum(decay_pre, 0.0) + jnp.log1p(jnp.exp(-jnp.abs(decay_pre)))
        decays.append(-rate * soft + extra)
        betas.append(jax.nn.sigmoid(beta_pre + bias))
    running = jnp.dot(
        jnp.concatenate(decays, axis=0), upto, precision=HIGH, preferred_element_type=F32
    )
    beta = jnp.concatenate(betas, axis=0)
    units = 2 * blocks
    tall = jnp.concatenate([running, beta, jnp.zeros((BLOCK - 2 * units, BLOCK), F32)], axis=0)
    columns = tall.T
    for which in range(2):
        maps = []
        for b in range(blocks):
            u = which * blocks + b
            pre = acc[which, BLOCK * b : BLOCK * (b + 1), :]
            act = pre * jax.nn.sigmoid(pre)
            key, value = act[:, :DK], act[:, DK:]
            key = key * lax.rsqrt(jnp.sum(key * key, axis=1, keepdims=True) + EPS)
            run_row = jnp.broadcast_to(running[u : u + 1, :], (BLOCK, BLOCK))
            run_col = jnp.broadcast_to(columns[:, u : u + 1], (BLOCK, BLOCK))
            beta_col = jnp.broadcast_to(columns[:, units + u : units + u + 1], (BLOCK, BLOCK))
            last = jnp.broadcast_to(running[u : u + 1, BLOCK - 1 :], (BLOCK, BLOCK))
            split = halves(key)
            gram = dot3(split, split, NT)
            strict = row > col
            weights = jnp.exp(jnp.where(strict, run_col - run_row, 0.0))
            low = jnp.where(strict, gram * beta_col * weights, 0.0)
            inverse = unit_lower_inverse(low, row, col).astype(BF16)
            right = jnp.concatenate([key * (beta_col * jnp.exp(run_col)), value * beta_col], axis=1)
            solved = dot1(inverse, right.astype(BF16))
            rest = right - solved - dot3(low, solved)
            solved = solved + dot1(inverse, rest.astype(BF16))
            late = key * jnp.exp(last - run_col)
            made = dot3(late.T, solved)
            keep = jnp.where(row == col, jnp.exp(last), 0.0)
            maps.append(jnp.concatenate([keep - made[:, :DK], made[:, DK:]], axis=1))
        while len(maps) > 1:
            maps = [composed(maps[i], maps[i + 1]) for i in range(0, len(maps), 2)]
        (mine, other)[which][...] = maps[0]


def composed(earlier, later):
    both = dot3(later[:, :DK], earlier)
    return jnp.concatenate([both[:, :DK], both[:, DK:] + later[:, DK:]], axis=1)


def local_maps(xg, w_key, w_value, w_other, gate_rows):
    _, rows, _ = xg.shape
    used = rows - PAD
    shape = jax.ShapeDtypeStruct((DK, DK + DV), F32)
    return pl.pallas_call(
        map_kernel,
        in_specs=[VMEM] * 5,
        out_specs=[VMEM] * 2,
        out_shape=[shape] * 2,
        scratch_shapes=[
            pltpu.VMEM((2, used, DK + DV), F32),
            pltpu.VMEM((gate_rows.shape[0], used), F32),
        ],
        compiler_params=granted(24),
    )(xg, w_key, w_value, w_other, gate_rows)


def in_order(mine, other, late):
    earlier = jnp.where(late, other, mine)
    later = jnp.where(late, mine, other)
    return composed(earlier, later)


def pair_kernel(mine, other, out):
    out[...] = in_order(mine[...], other[...], lax.axis_index("tp") % 2 == 1)


def pair_composed(mine, other):
    return pl.pallas_call(
        pair_kernel,
        in_specs=[VMEM] * 2,
        out_specs=VMEM,
        out_shape=jax.ShapeDtypeStruct(mine.shape, F32),
        compiler_params=granted(4),
    )(mine, other)


QUARTER = 32


def couple_kernel(mine, other, keep, give):
    place = lax.axis_index("sp")
    whole = in_order(mine[...], other[...], place % 2 == 1)
    keep[...] = whole
    core = place % 2

    @pl.when((place // 2) % 2 == 0)
    def _():
        give[...] = whole[:, DK:]

    @pl.when((place // 2) % 2 == 1)
    def _():
        mine_rows = pl.ds(pl.multiple_of(core * QUARTER, QUARTER), QUARTER)
        give[0:QUARTER, :] = keep[mine_rows, :DK]
        give[QUARTER : 2 * QUARTER, :] = keep[mine_rows, DK:]
        give[2 * QUARTER :, :] = jnp.zeros((DK - 2 * QUARTER, DV), F32)


def coupled(mine, other):
    return pl.pallas_call(
        couple_kernel,
        in_specs=[VMEM] * 2,
        out_specs=[VMEM] * 2,
        out_shape=[jax.ShapeDtypeStruct(mine.shape, F32), jax.ShapeDtypeStruct((DK, DV), F32)],
        compiler_params=granted(4),
    )(mine, other)


def owner_kernel(keep, got, query, state, read):
    place = lax.axis_index("sp")
    late = (place // 2) % 2 == 1
    core = place % 2
    rows = pl.ds(pl.multiple_of(2 * QUARTER + core * QUARTER, QUARTER), QUARTER)
    early = jnp.where(late, got[...], keep[:, DK:])
    last_map = jnp.where(late, keep[rows, :DK], got[0:QUARTER, :])
    last_add = jnp.where(late, keep[rows, DK:], got[QUARTER : 2 * QUARTER, :])
    owned = (dot3(last_map, early) + last_add).astype(BF16)
    state[...] = owned
    which = lax.broadcasted_iota(jnp.int32, query.shape, 0)
    lane = lax.broadcasted_iota(jnp.int32, query.shape, 1)
    chosen = (which == place // 4) & (lane // QUARTER == place % 4)
    picked = jnp.where(chosen, query[...].astype(F32), 0.0).astype(BF16)
    tall = jnp.concatenate([owned] * (DK // QUARTER), axis=0)
    read[...] = jnp.sum(dot1(picked, tall), axis=0, keepdims=True)


def owner_rows(keep, got, query):
    return pl.pallas_call(
        owner_kernel,
        in_specs=[VMEM] * 3,
        out_specs=[VMEM] * 2,
        out_shape=[jax.ShapeDtypeStruct((QUARTER, DV), BF16), jax.ShapeDtypeStruct((1, DV), F32)],
        compiler_params=granted(4),
    )(keep, got, query)


def shards(
    layer_input,
    w_key,
    w_value,
    w_gates,
    decay_rate,
    beta_bias,
    log_decay_extra,
    new_query,
    read_gain,
):
    prompts, _, _ = layer_input.shape
    sp = lax.axis_size("sp")
    tp = lax.axis_size("tp")
    chunks = sp // prompts
    pair = [(i, i ^ 1) for i in range(tp)]
    w_other = lax.ppermute(jnp.stack([w_key, w_value]), "tp", pair)

    sent = packed(layer_input, log_decay_extra[:, 0, :])
    groups = [[prompts * t + j for j in range(prompts)] for t in range(chunks)]
    here = lax.all_to_all(sent, "sp", 0, 0, axis_index_groups=groups, tiled=True)

    parcel = parcels(here, decay_rate, beta_bias, tp)
    gathered = lax.all_to_all(parcel, "tp", 0, 0, tiled=True)

    gate_rows = w_gates.transpose(0, 2, 1).reshape(2 * tp, -1)
    mine, theirs = local_maps(gathered, w_key, w_value, w_other, gate_rows)
    other = lax.ppermute(theirs, "tp", pair)
    whole = pair_composed(mine, other)

    moved = lax.ppermute(
        whole, "sp", [(prompts * t + j, chunks * j + t) for t in range(chunks) for j in range(prompts)]
    )
    near = lax.ppermute(moved, "sp", [(i, i ^ 1) for i in range(sp)])
    keep, give = coupled(moved, near)
    got = lax.ppermute(give, "sp", [(i, i ^ 2) for i in range(sp)])
    state_cache, partial = owner_rows(keep, got, new_query)

    parts = lax.all_to_all(
        jnp.broadcast_to(partial[None], (sp, 1, DV)), "sp", 0, 0, tiled=True
    )
    raw = parts.reshape(prompts, chunks, DV).sum(axis=1)
    scaled = raw * lax.rsqrt(jnp.mean(raw * raw, axis=-1, keepdims=True) + EPS) * read_gain
    return state_cache, scaled.astype(BF16)


def solution(mesh):
    placed = (
        P(None, "sp", "tp"),
        P(None, "tp"),
        P(None, "tp"),
        P(),
        P("tp"),
        P("tp"),
        P(None, "tp", "sp"),
        P(None, "tp"),
        P(),
    )

    return jax.shard_map(
        shards, mesh=mesh, in_specs=placed, out_specs=(P("sp", "tp"), P(None, "tp")), check_vma=False
    )
```

```python
import jax
import jax.numpy as jnp
from jax import lax
from jax.experimental import pallas as pl
from jax.experimental.pallas import tpu as pltpu
from jax.sharding import PartitionSpec as P


DK = 128
DV = 128
BLOCK = 128
EPS = 1e-06
HIGH = lax.Precision.HIGHEST
F32 = jnp.float32
BF16 = jnp.bfloat16
PAD = 16
SHIFT = 5


MIB = 1 << 20
VMEM = pl.BlockSpec(memory_space=pltpu.VMEM)
SMEM = pl.BlockSpec(memory_space=pltpu.SMEM)


def granted(mib):
    return pltpu.CompilerParams(vmem_limit_bytes=mib * MIB)


NN = (((1,), (0,)), ((), ()))
NT = (((1,), (1,)), ((), ()))


def dot1(left, right, dims=NN):
    return lax.dot_general(left, right, dims, preferred_element_type=F32)


def halves(x):
    high = x.astype(BF16)
    low = (x - high.astype(F32)).astype(BF16)
    return high, low


def dot3(left, right, dims=NN):
    (la,), (ra,) = dims[0]
    lh, ll = halves(left)
    rh, rl = halves(right)
    return dot1(
        jnp.concatenate([lh, ll, lh], axis=la), jnp.concatenate([rh, rh, rl], axis=ra), dims
    )


MIB = 1 << 20
VMEM = pl.BlockSpec(memory_space=pltpu.VMEM)
SMEM = pl.BlockSpec(memory_space=pltpu.SMEM)


def granted(mib):
    return pltpu.CompilerParams(vmem_limit_bytes=mib * MIB)


NN = (((1,), (0,)), ((), ()))
NT = (((1,), (1,)), ((), ()))


def dot1(left, right, dims=NN):
    return lax.dot_general(left, right, dims, preferred_element_type=F32)


def halves(x):
    high = x.astype(BF16)
    low = (x - high.astype(F32)).astype(BF16)
    return high, low


def dot3(left, right, dims=NN):
    (la,), (ra,) = dims[0]
    lh, ll = halves(left)
    rh, rl = halves(right)
    return dot1(
        jnp.concatenate([lh, ll, lh], axis=la), jnp.concatenate([rh, rh, rl], axis=ra), dims
    )


def three_pieces(x):
    high = x.astype(BF16).astype(F32)
    rest = x - high
    mid = rest.astype(BF16).astype(F32)
    return high, mid, (rest - mid).astype(BF16).astype(F32)


def pack_kernel(x, extra, out):
    prompts, seg, width = x.shape
    first = lax.axis_index("sp") // prompts * 2 + SHIFT
    for i in range(prompts):
        prompt = lax.rem(first + i, prompts)
        out[i, :seg, :] = x[prompt]
        rows = list(three_pieces(extra[pl.ds(prompt, 1), :])) + [jnp.zeros((PAD - 3, width), F32)]
        out[i, seg:, :] = jnp.concatenate(rows, axis=0).astype(BF16)


def packed(layer_input, extra):
    prompts, seg, width = layer_input.shape
    return pl.pallas_call(
        pack_kernel,
        in_specs=[VMEM, VMEM],
        out_specs=VMEM,
        out_shape=jax.ShapeDtypeStruct((prompts, seg + PAD, width), BF16),
        compiler_params=granted(4),
    )(layer_input, extra)


def parcel_kernel(here, rate, bias, out):
    segs, rows, width = here.shape
    seg = rows - PAD
    half = segs // 2
    lane = lax.broadcasted_iota(jnp.int32, (1, width), 1)
    consts = three_pieces(jnp.where(lane < width // 2, rate[0], bias[0]))
    for which in range(2):
        tails = [here[half * which + b, seg:, :].astype(F32) for b in range(half)]
        tail = [tails[b][i : i + 1] for i in range(3) for b in range(half)]
        tail = jnp.concatenate(tail + list(consts) + [jnp.zeros((PAD - 3 * half - 3, width), F32)], axis=0)
        tail = tail.astype(BF16)
        body = [here[half * which + b, :seg, :] for b in range(half)]
        for other in range(which, out.shape[0], 2):
            for b in range(half):
                out[other, seg * b : seg * (b + 1), :] = body[b]
            out[other, seg * half :, :] = tail


def parcels(here, rate, bias, count):
    segs, rows, width = here.shape
    return pl.pallas_call(
        parcel_kernel,
        in_specs=[VMEM, SMEM, SMEM],
        out_specs=VMEM,
        out_shape=jax.ShapeDtypeStruct((count, (segs // 2) * (rows - PAD) + PAD, width), BF16),
        compiler_params=granted(8),
    )(here, rate, bias)


def invert_unit_lower(low, inverse, product, row, col):
    units, size, _ = low.shape
    step = 1
    while step < size:
        merge = ((row // (2 * step)) == (col // (2 * step))) & ((row // step) != (col // step))
        if step == 1:
            eye = (row == col).astype(F32)
            for u in range(units):
                part = jnp.where(merge, low[u].astype(F32), 0.0)
                inverse[u] = (eye - part).astype(BF16)
        else:
            if step < 16:
                lower_rows = [(0, size)]
            else:
                lower_rows = [(at, step) for at in range(step, size, 2 * step)]
            rows = sum(length for _, length in lower_rows)
            take = lambda u: jnp.concatenate([inverse[u, at : at + n, :] for at, n in lower_rows], axis=0)
            for u in range(units):
                part = jnp.where(merge, low[u].astype(F32), 0.0).astype(BF16)
                product[u, :rows, :] = dot1(take(u), part).astype(BF16)
            for u in range(units):
                fill = dot1(product[u, :rows, :], inverse[u])
                fill = (take(u).astype(F32) - fill).astype(BF16)
                done = 0
                for at, n in lower_rows:
                    inverse[u, at : at + n, :] = fill[done : done + n]
                    done += n
        step *= 2


def map_kernel(
    xg, wk, wv, wok, wov, wg, mine, other, acc, gates, keys, low, low_rest, inverse, product, right, solved, maps
):
    sources, rows, width = xg.shape
    rows = rows - PAD
    blocks = rows // BLOCK
    units = 2 * blocks
    me = lax.axis_index("tp")
    x = jnp.concatenate([xg[i, :rows, :] for i in range(sources)], axis=1)
    gates[...] = dot1(wg[...], x, NT)
    acc[0] = dot1(x, jnp.concatenate([wk[...], wv[...]], axis=1))
    acc[1] = dot1(x, jnp.concatenate([wok[...], wov[...]], axis=1))

    row = lax.broadcasted_iota(jnp.int32, (BLOCK, BLOCK), 0)
    col = lax.broadcasted_iota(jnp.int32, (BLOCK, BLOCK), 1)
    upto = (row <= col).astype(F32)
    strict = row > col
    decays, betas = [], []
    for which in range(2):
        head = me if which == 0 else me ^ 1
        extras = xg[head, rows:, :].astype(F32)
        extra = extras[0:4] + extras[4:8] + extras[8:12]
        consts = extras[12:13] + extras[13:14] + extras[14:15]
        rate, bias = consts[:, 0:1], consts[:, width // 2 : width // 2 + 1]
        cut = lambda g: jnp.concatenate(
            [g[:, BLOCK * b : BLOCK * (b + 1)] for b in range(blocks)], axis=0
        )
        decay_pre = cut(gates[pl.ds(head, 1), :])
        beta_pre = cut(gates[pl.ds(sources + head, 1), :])
        soft = jnp.maximum(decay_pre, 0.0) + jnp.log1p(jnp.exp(-jnp.abs(decay_pre)))
        decays.append(-rate * soft + extra)
        betas.append(jax.nn.sigmoid(beta_pre + bias))
    running = jnp.dot(
        jnp.concatenate(decays, axis=0), upto, precision=HIGH, preferred_element_type=F32
    )
    beta = jnp.concatenate(betas, axis=0)
    tall = jnp.concatenate([running, beta, jnp.zeros((BLOCK - 2 * units, BLOCK), F32)], axis=0)
    columns = tall.T
    run_col = lambda u: jnp.broadcast_to(columns[:, u : u + 1], (BLOCK, BLOCK))
    beta_col = lambda u: jnp.broadcast_to(columns[:, units + u : units + u + 1], (BLOCK, BLOCK))
    run_row = lambda u: jnp.broadcast_to(running[u : u + 1, :], (BLOCK, BLOCK))
    last = lambda u: jnp.broadcast_to(running[u : u + 1, BLOCK - 1 :], (BLOCK, BLOCK))
    for u in range(units):
        which, b = divmod(u, blocks)
        pre = acc[which, BLOCK * b : BLOCK * (b + 1), :]
        act = pre * jax.nn.sigmoid(pre)
        key, value = act[:, :DK], act[:, DK:]
        key = key * lax.rsqrt(jnp.sum(key * key, axis=1, keepdims=True) + EPS)
        keys[u] = key
        strength = beta_col(u)
        right[u, :, :DK] = key * (strength * jnp.exp(run_col(u)))
        right[u, :, DK:] = value * strength
    for u in range(units):
        key = keys[u]
        gram = dot3(key, key, NT)
        weights = jnp.exp(jnp.where(strict, run_col(u) - run_row(u), 0.0))
        high, rest = halves(jnp.where(strict, gram * beta_col(u) * weights, 0.0))
        low[u] = high
        low_rest[u] = rest
    invert_unit_lower(low, inverse, product, row, col)
    for u in range(units):
        solved[u] = dot1(inverse[u], right[u].astype(BF16)).astype(BF16)
    for u in range(units):
        first = solved[u]
        taken = dot1(
            jnp.concatenate([low[u], low_rest[u]], axis=1), jnp.concatenate([first, first], axis=0)
        )
        right[u] = right[u] - first.astype(F32) - taken
    for u in range(units):
        right[u] = solved[u].astype(F32) + dot1(inverse[u], right[u].astype(BF16))
    for u in range(units):
        late = keys[u] * jnp.exp(last(u) - run_col(u))
        made = dot3(late.T, right[u])
        keep = jnp.where(row == col, jnp.exp(last(u)), 0.0)
        maps[u, :, :DK] = keep - made[:, :DK]
        maps[u, :, DK:] = made[:, DK:]
    apart = 1
    while apart < blocks:
        for u in range(0, units, 2 * apart):
            result = composed(maps[u], maps[u + apart])
            if 2 * apart < blocks:
                maps[u] = result
            else:
                (mine, other)[u // blocks][...] = result
        apart *= 2


def composed(earlier, later):
    both = dot3(later[:, :DK], earlier)
    return jnp.concatenate([both[:, :DK], both[:, DK:] + later[:, DK:]], axis=1)


def local_maps(xg, w_key, w_value, other_key, other_value, gate_rows):
    _, rows, _ = xg.shape
    used = rows - PAD
    units = 2 * (used // BLOCK)
    shape = jax.ShapeDtypeStruct((DK, DK + DV), F32)
    return pl.pallas_call(
        map_kernel,
        in_specs=[VMEM] * 6,
        out_specs=[VMEM] * 2,
        out_shape=[shape] * 2,
        scratch_shapes=[
            pltpu.VMEM((2, used, DK + DV), F32),
            pltpu.VMEM((gate_rows.shape[0], used), F32),
            pltpu.VMEM((units, BLOCK, DK), F32),
            pltpu.VMEM((units, BLOCK, BLOCK), BF16),
            pltpu.VMEM((units, BLOCK, BLOCK), BF16),
            pltpu.VMEM((units, BLOCK, BLOCK), BF16),
            pltpu.VMEM((units, BLOCK, BLOCK), BF16),
            pltpu.VMEM((units, BLOCK, DK + DV), F32),
            pltpu.VMEM((units, BLOCK, DK + DV), BF16),
            pltpu.VMEM((units, DK, DK + DV), F32),
        ],
        compiler_params=granted(28),
    )(xg, w_key, w_value, other_key, other_value, gate_rows)


def in_order(mine, other, late):
    earlier = jnp.where(late, other, mine)
    later = jnp.where(late, mine, other)
    return composed(earlier, later)


def pair_kernel(mine, other, out):
    out[...] = in_order(mine[...], other[...], lax.axis_index("tp") % 2 == 1)


def pair_composed(mine, other):
    return pl.pallas_call(
        pair_kernel,
        in_specs=[VMEM] * 2,
        out_specs=VMEM,
        out_shape=jax.ShapeDtypeStruct(mine.shape, F32),
        compiler_params=granted(4),
    )(mine, other)


QUARTER = 32


def couple_kernel(mine, other, keep, give):
    place = lax.axis_index("sp")
    whole = in_order(mine[...], other[...], place % 2 == 1)
    keep[...] = whole
    core = place % 2

    @pl.when((place // 2) % 2 == 0)
    def _():
        give[...] = whole[:, DK:]

    @pl.when((place // 2) % 2 == 1)
    def _():
        mine_rows = pl.ds(pl.multiple_of(core * QUARTER, QUARTER), QUARTER)
        give[0:QUARTER, :] = keep[mine_rows, :DK]
        give[QUARTER : 2 * QUARTER, :] = keep[mine_rows, DK:]
        give[2 * QUARTER :, :] = jnp.zeros((DK - 2 * QUARTER, DV), F32)


def coupled(mine, other):
    return pl.pallas_call(
        couple_kernel,
        in_specs=[VMEM] * 2,
        out_specs=[VMEM] * 2,
        out_shape=[jax.ShapeDtypeStruct(mine.shape, F32), jax.ShapeDtypeStruct((DK, DV), F32)],
        compiler_params=granted(4),
    )(mine, other)


def owner_kernel(keep, got, query, state, read):
    place = lax.axis_index("sp")
    late = (place // 2) % 2 == 1
    core = place % 2
    rows = pl.ds(pl.multiple_of(2 * QUARTER + core * QUARTER, QUARTER), QUARTER)
    early = jnp.where(late, got[...], keep[:, DK:])
    last_map = jnp.where(late, keep[rows, :DK], got[0:QUARTER, :])
    last_add = jnp.where(late, keep[rows, DK:], got[QUARTER : 2 * QUARTER, :])
    owned = (dot3(last_map, early) + last_add).astype(BF16)
    state[...] = owned
    which = lax.broadcasted_iota(jnp.int32, query.shape, 0)
    lane = lax.broadcasted_iota(jnp.int32, query.shape, 1)
    chosen = (which == place // 4) & (lane // QUARTER == place % 4)
    picked = jnp.where(chosen, query[...].astype(F32), 0.0).astype(BF16)
    tall = jnp.concatenate([owned] * (DK // QUARTER), axis=0)
    read[...] = jnp.sum(dot1(picked, tall), axis=0, keepdims=True)


def owner_rows(keep, got, query):
    return pl.pallas_call(
        owner_kernel,
        in_specs=[VMEM] * 3,
        out_specs=[VMEM] * 2,
        out_shape=[jax.ShapeDtypeStruct((QUARTER, DV), BF16), jax.ShapeDtypeStruct((1, DV), F32)],
        compiler_params=granted(4),
    )(keep, got, query)


def shards(
    layer_input,
    w_key,
    w_value,
    w_gates,
    decay_rate,
    beta_bias,
    log_decay_extra,
    new_query,
    read_gain,
):
    prompts, _, _ = layer_input.shape
    sp = lax.axis_size("sp")
    tp = lax.axis_size("tp")
    chunks = sp // prompts
    pair = [(i, i ^ 1) for i in range(tp)]
    other_key = lax.ppermute(w_key, "tp", pair)
    other_value = lax.ppermute(w_value, "tp", pair)

    sent = packed(layer_input, log_decay_extra[:, 0, :])
    groups = [[prompts * t + j for j in range(prompts)] for t in range(chunks)]
    here = lax.all_to_all(sent, "sp", 0, 0, axis_index_groups=groups, tiled=True)

    parcel = parcels(here, decay_rate, beta_bias, tp)
    gathered = lax.all_to_all(parcel, "tp", 0, 0, tiled=True)

    gate_rows = w_gates.transpose(0, 2, 1).reshape(2 * tp, -1)
    mine, theirs = local_maps(gathered, w_key, w_value, other_key, other_value, gate_rows)
    other = lax.ppermute(theirs, "tp", pair)
    whole = pair_composed(mine, other)

    ways = [
        (prompts * t + i, chunks * ((2 * t + SHIFT + i) % prompts) + t)
        for t in range(chunks)
        for i in range(prompts)
    ]
    moved = lax.ppermute(whole, "sp", ways)
    near = lax.ppermute(moved, "sp", [(i, i ^ 1) for i in range(sp)])
    keep, give = coupled(moved, near)
    got = lax.ppermute(give, "sp", [(i, i ^ 2) for i in range(sp)])
    state_cache, partial = owner_rows(keep, got, new_query)

    parts = lax.all_to_all(
        jnp.broadcast_to(partial[None], (sp, 1, DV)), "sp", 0, 0, tiled=True
    )
    raw = parts.reshape(prompts, chunks, DV).sum(axis=1)
    scaled = raw * lax.rsqrt(jnp.mean(raw * raw, axis=-1, keepdims=True) + EPS) * read_gain
    return state_cache, scaled.astype(BF16)


def solution(mesh):
    placed = (
        P(None, "sp", "tp"),
        P(None, "tp"),
        P(None, "tp"),
        P(),
        P("tp"),
        P("tp"),
        P(None, "tp", "sp"),
        P(None, "tp"),
        P(),
    )

    return jax.shard_map(
        shards, mesh=mesh, in_specs=placed, out_specs=(P("sp", "tp"), P(None, "tp")), check_vma=False
    )
```

```python
import jax
import jax.numpy as jnp
from jax import lax
from jax.experimental import pallas as pl
from jax.experimental.pallas import tpu as pltpu
from jax.sharding import PartitionSpec as P


DK = 128
DV = 128
BLOCK = 128
EPS = 1e-06
HIGH = lax.Precision.HIGHEST
F32 = jnp.float32
BF16 = jnp.bfloat16
PAD = 16
SHIFT = 5


MIB = 1 << 20
VMEM = pl.BlockSpec(memory_space=pltpu.VMEM)
SMEM = pl.BlockSpec(memory_space=pltpu.SMEM)
HBM = pl.BlockSpec(memory_space=pltpu.HBM)


def granted(mib):
    return pltpu.CompilerParams(vmem_limit_bytes=mib * MIB)


NN = (((1,), (0,)), ((), ()))
NT = (((1,), (1,)), ((), ()))


def dot1(left, right, dims=NN):
    return lax.dot_general(left, right, dims, preferred_element_type=F32)


def halves(x):
    high = x.astype(BF16)
    low = (x - high.astype(F32)).astype(BF16)
    return high, low


def dot3(left, right, dims=NN):
    (la,), (ra,) = dims[0]
    lh, ll = halves(left)
    rh, rl = halves(right)
    return dot1(
        jnp.concatenate([lh, ll, lh], axis=la), jnp.concatenate([rh, rh, rl], axis=ra), dims
    )


MIB = 1 << 20
VMEM = pl.BlockSpec(memory_space=pltpu.VMEM)
SMEM = pl.BlockSpec(memory_space=pltpu.SMEM)
HBM = pl.BlockSpec(memory_space=pltpu.HBM)


def granted(mib):
    return pltpu.CompilerParams(vmem_limit_bytes=mib * MIB)


NN = (((1,), (0,)), ((), ()))
NT = (((1,), (1,)), ((), ()))


def dot1(left, right, dims=NN):
    return lax.dot_general(left, right, dims, preferred_element_type=F32)


def halves(x):
    high = x.astype(BF16)
    low = (x - high.astype(F32)).astype(BF16)
    return high, low


def dot3(left, right, dims=NN):
    (la,), (ra,) = dims[0]
    lh, ll = halves(left)
    rh, rl = halves(right)
    return dot1(
        jnp.concatenate([lh, ll, lh], axis=la), jnp.concatenate([rh, rh, rl], axis=ra), dims
    )


def three_pieces(x):
    high = x.astype(BF16).astype(F32)
    rest = x - high
    mid = rest.astype(BF16).astype(F32)
    return high, mid, (rest - mid).astype(BF16).astype(F32)


def pack_kernel(x, extra, out, held, sem):
    prompts, seg, width = x.shape
    first = lax.axis_index("sp") // prompts * 2 + SHIFT
    which = lambda i: lax.rem(first + i, prompts)
    copies = [
        pltpu.make_async_copy(x.at[which(i)], out.at[i, pl.ds(0, seg)], sem.at[i])
        for i in range(prompts)
    ]
    copies.append(pltpu.make_async_copy(extra, held, sem.at[prompts]))
    for copy in reversed(copies):
        copy.start()
    copies[-1].wait()
    for i in range(prompts):
        rows = list(three_pieces(held[pl.ds(which(i), 1), :])) + [jnp.zeros((PAD - 3, width), F32)]
        out[i, seg:, :] = jnp.concatenate(rows, axis=0).astype(BF16)
    for copy in copies[:-1]:
        copy.wait()


def packed(layer_input, extra):
    prompts, seg, width = layer_input.shape
    return pl.pallas_call(
        pack_kernel,
        in_specs=[HBM, HBM],
        out_specs=VMEM,
        out_shape=jax.ShapeDtypeStruct((prompts, seg + PAD, width), BF16),
        scratch_shapes=[pltpu.VMEM(extra.shape, F32), pltpu.SemaphoreType.DMA((prompts + 1,))],
        compiler_params=granted(60),
    )(layer_input, extra)


def parcel_kernel(here, rate, bias, out):
    segs, rows, width = here.shape
    seg = rows - PAD
    half = segs // 2
    lane = lax.broadcasted_iota(jnp.int32, (1, width), 1)
    consts = three_pieces(jnp.where(lane < width // 2, rate[0], bias[0]))
    for which in range(2):
        tails = [here[half * which + b, seg:, :].astype(F32) for b in range(half)]
        tail = [tails[b][i : i + 1] for i in range(3) for b in range(half)]
        tail = jnp.concatenate(tail + list(consts) + [jnp.zeros((PAD - 3 * half - 3, width), F32)], axis=0)
        tail = tail.astype(BF16)
        body = [here[half * which + b, :seg, :] for b in range(half)]
        for other in range(which, out.shape[0], 2):
            for b in range(half):
                out[other, seg * b : seg * (b + 1), :] = body[b]
            out[other, seg * half :, :] = tail


def parcels(here, rate, bias, count):
    segs, rows, width = here.shape
    return pl.pallas_call(
        parcel_kernel,
        in_specs=[VMEM, SMEM, SMEM],
        out_specs=VMEM,
        out_shape=jax.ShapeDtypeStruct((count, (segs // 2) * (rows - PAD) + PAD, width), BF16),
        compiler_params=granted(8),
    )(here, rate, bias)


def invert_unit_lower(low, inverse, product, row, col):
    units, size, _ = low.shape
    step = 1
    while step < size:
        merge = ((row // (2 * step)) == (col // (2 * step))) & ((row // step) != (col // step))
        if step == 1:
            eye = (row == col).astype(F32)
            for u in range(units):
                part = jnp.where(merge, low[u].astype(F32), 0.0)
                inverse[u] = (eye - part).astype(BF16)
        else:
            if step < 16:
                lower_rows = [(0, size)]
            else:
                lower_rows = [(at, step) for at in range(step, size, 2 * step)]
            rows = sum(length for _, length in lower_rows)
            take = lambda u: jnp.concatenate([inverse[u, at : at + n, :] for at, n in lower_rows], axis=0)
            for u in range(units):
                part = jnp.where(merge, low[u].astype(F32), 0.0).astype(BF16)
                product[u, :rows, :] = dot1(take(u), part).astype(BF16)
            for u in range(units):
                fill = dot1(product[u, :rows, :], inverse[u])
                fill = (take(u).astype(F32) - fill).astype(BF16)
                done = 0
                for at, n in lower_rows:
                    inverse[u, at : at + n, :] = fill[done : done + n]
                    done += n
        step *= 2


def partner_kernel(xg, first, second, wg, out, gates, *scratch):
    *scratch, weights, sem = scratch
    core = lax.axis_index("sp") % 2
    copies = [
        pltpu.make_async_copy(first, weights.at[core], sem.at[0]),
        pltpu.make_async_copy(second, weights.at[1 - core], sem.at[1]),
    ]
    for copy in copies:
        copy.start()
    x = features(xg)
    gates[...] = dot1(wg[...], x, NT)
    for copy in copies:
        copy.wait()
    head_map(lax.axis_index("tp") ^ 1, x, xg, weights[0], weights[1], gates, out, *scratch)


def own_kernel(xg, w_key, w_value, gates, out, *scratch):
    head_map(lax.axis_index("tp"), features(xg), xg, w_key[...], w_value[...], gates, out, *scratch)


def features(xg):
    sources, rows, _ = xg.shape
    return jnp.concatenate([xg[i, : rows - PAD, :] for i in range(sources)], axis=1)


def head_map(head, x, xg, w_key, w_value, gates, out, acc, keys, low, low_rest, inverse, product, right, solved, maps):
    sources, rows, width = xg.shape
    rows = rows - PAD
    blocks = units = rows // BLOCK
    acc[...] = dot1(x, jnp.concatenate([w_key, w_value], axis=1))

    row = lax.broadcasted_iota(jnp.int32, (BLOCK, BLOCK), 0)
    col = lax.broadcasted_iota(jnp.int32, (BLOCK, BLOCK), 1)
    upto = (row <= col).astype(F32)
    strict = row > col
    extras = xg[head, rows:, :].astype(F32)
    extra = extras[0:4] + extras[4:8] + extras[8:12]
    consts = extras[12:13] + extras[13:14] + extras[14:15]
    rate, bias = consts[:, 0:1], consts[:, width // 2 : width // 2 + 1]
    cut = lambda g: jnp.concatenate([g[:, BLOCK * b : BLOCK * (b + 1)] for b in range(blocks)], axis=0)
    decay_pre = cut(gates[pl.ds(head, 1), :])
    beta_pre = cut(gates[pl.ds(sources + head, 1), :])
    soft = jnp.maximum(decay_pre, 0.0) + jnp.log1p(jnp.exp(-jnp.abs(decay_pre)))
    beta = jax.nn.sigmoid(beta_pre + bias)
    decay = jnp.concatenate([-rate * soft + extra, jnp.zeros((8 - blocks, BLOCK), F32)], axis=0)
    running = jnp.dot(decay, upto, precision=HIGH, preferred_element_type=F32)[:units]
    tall = jnp.concatenate([running, beta, jnp.zeros((BLOCK - 2 * units, BLOCK), F32)], axis=0)
    columns = tall.T
    run_col = lambda u: jnp.broadcast_to(columns[:, u : u + 1], (BLOCK, BLOCK))
    beta_col = lambda u: jnp.broadcast_to(columns[:, units + u : units + u + 1], (BLOCK, BLOCK))
    run_row = lambda u: jnp.broadcast_to(running[u : u + 1, :], (BLOCK, BLOCK))
    last = lambda u: jnp.broadcast_to(running[u : u + 1, BLOCK - 1 :], (BLOCK, BLOCK))
    for u in range(units):
        pre = acc[BLOCK * u : BLOCK * (u + 1), :]
        act = pre * jax.nn.sigmoid(pre)
        key, value = act[:, :DK], act[:, DK:]
        key = key * lax.rsqrt(jnp.sum(key * key, axis=1, keepdims=True) + EPS)
        keys[u] = key
        strength = beta_col(u)
        right[u, :, :DK] = key * (strength * jnp.exp(run_col(u)))
        right[u, :, DK:] = value * strength
    for u in range(units):
        key = keys[u]
        gram = dot3(key, key, NT)
        weights = jnp.exp(jnp.where(strict, run_col(u) - run_row(u), 0.0))
        high, rest = halves(jnp.where(strict, gram * beta_col(u) * weights, 0.0))
        low[u] = high
        low_rest[u] = rest
    invert_unit_lower(low, inverse, product, row, col)
    for u in range(units):
        solved[u] = dot1(inverse[u], right[u].astype(BF16)).astype(BF16)
    for u in range(units):
        first = solved[u]
        taken = dot1(
            jnp.concatenate([low[u], low_rest[u]], axis=1), jnp.concatenate([first, first], axis=0)
        )
        right[u] = right[u] - first.astype(F32) - taken
    for u in range(units):
        right[u] = solved[u].astype(F32) + dot1(inverse[u], right[u].astype(BF16))
    for u in range(units):
        late = keys[u] * jnp.exp(last(u) - run_col(u))
        made = dot3(late.T, right[u])
        keep = jnp.where(row == col, jnp.exp(last(u)), 0.0)
        maps[u, :, :DK] = keep - made[:, :DK]
        maps[u, :, DK:] = made[:, DK:]
    apart = 1
    while apart < blocks:
        for u in range(0, units, 2 * apart):
            result = composed(maps[u], maps[u + apart])
            if 2 * apart < blocks:
                maps[u] = result
            else:
                out[...] = result
        apart *= 2


def composed(earlier, later):
    both = dot3(later[:, :DK], earlier)
    return jnp.concatenate([both[:, :DK], both[:, DK:] + later[:, DK:]], axis=1)


def head_call(kernel, outs, more, used, specs, *operands):
    units = used // BLOCK
    shape = jax.ShapeDtypeStruct((DK, DK + DV), F32)
    return pl.pallas_call(
        kernel,
        in_specs=specs,
        out_specs=[VMEM] * (1 + len(outs)),
        out_shape=[shape, *outs],
        scratch_shapes=[
            pltpu.VMEM((used, DK + DV), F32),
            pltpu.VMEM((units, BLOCK, DK), F32),
            pltpu.VMEM((units, BLOCK, BLOCK), BF16),
            pltpu.VMEM((units, BLOCK, BLOCK), BF16),
            pltpu.VMEM((units, BLOCK, BLOCK), BF16),
            pltpu.VMEM((units, BLOCK, BLOCK), BF16),
            pltpu.VMEM((units, BLOCK, DK + DV), F32),
            pltpu.VMEM((units, BLOCK, DK + DV), BF16),
            pltpu.VMEM((units, DK, DK + DV), F32),
            *more,
        ],
        compiler_params=granted(24),
    )(*operands)


def in_order(mine, other, late):
    earlier = jnp.where(late, other, mine)
    later = jnp.where(late, mine, other)
    return composed(earlier, later)


def diagonal():
    row = lax.broadcasted_iota(jnp.int32, (DK, DK), 0)
    return row == lax.broadcasted_iota(jnp.int32, (DK, DK), 1)


def pair_kernel(mine, other, out):
    whole = in_order(mine[...], other[...], lax.axis_index("tp") % 2 == 1)
    out[:DK, :] = whole.astype(BF16)
    part = whole[:, :DK]
    lost = part - part.astype(BF16).astype(F32)
    lost = jnp.sum(jnp.where(diagonal(), lost, 0.0), axis=0, keepdims=True)
    lost = jnp.concatenate([lost, jnp.zeros((PAD - 1, DK), F32)], axis=0)
    out[DK:, :] = jnp.concatenate([lost, jnp.zeros_like(lost)], axis=1).astype(BF16)


def widened(sent):
    whole = sent[:DK, :].astype(F32)
    lost = sent[DK:, :DK].astype(F32)[:1]
    part = whole[:, :DK] + jnp.where(diagonal(), jnp.broadcast_to(lost, (DK, DK)), 0.0)
    return jnp.concatenate([part, whole[:, DK:]], axis=1)


def pair_composed(mine, other):
    return pl.pallas_call(
        pair_kernel,
        in_specs=[VMEM] * 2,
        out_specs=VMEM,
        out_shape=jax.ShapeDtypeStruct((DK + PAD, DK + DV), BF16),
        compiler_params=granted(4),
    )(mine, other)


QUARTER = 32


def couple_kernel(mine, other, keep, give):
    place = lax.axis_index("sp")
    whole = in_order(widened(mine[...]), widened(other[...]), place % 2 == 1)
    keep[...] = whole
    core = place % 2

    @pl.when((place // 2) % 2 == 0)
    def _():
        give[...] = whole[:, DK:]

    @pl.when((place // 2) % 2 == 1)
    def _():
        mine_rows = pl.ds(pl.multiple_of(core * QUARTER, QUARTER), QUARTER)
        give[0:QUARTER, :] = keep[mine_rows, :DK]
        give[QUARTER : 2 * QUARTER, :] = keep[mine_rows, DK:]
        give[2 * QUARTER :, :] = jnp.zeros((DK - 2 * QUARTER, DV), F32)


def coupled(mine, other):
    return pl.pallas_call(
        couple_kernel,
        in_specs=[VMEM] * 2,
        out_specs=[VMEM] * 2,
        out_shape=[jax.ShapeDtypeStruct((DK, DK + DV), F32), jax.ShapeDtypeStruct((DK, DV), F32)],
        compiler_params=granted(4),
    )(mine, other)


def owner_kernel(keep, got, query, state, read):
    place = lax.axis_index("sp")
    late = (place // 2) % 2 == 1
    core = place % 2
    rows = pl.ds(pl.multiple_of(2 * QUARTER + core * QUARTER, QUARTER), QUARTER)
    early = jnp.where(late, got[...], keep[:, DK:])
    last_map = jnp.where(late, keep[rows, :DK], got[0:QUARTER, :])
    last_add = jnp.where(late, keep[rows, DK:], got[QUARTER : 2 * QUARTER, :])
    owned = (dot3(last_map, early) + last_add).astype(BF16)
    state[...] = owned
    which = lax.broadcasted_iota(jnp.int32, query.shape, 0)
    lane = lax.broadcasted_iota(jnp.int32, query.shape, 1)
    chosen = (which == place // 4) & (lane // QUARTER == place % 4)
    picked = jnp.where(chosen, query[...].astype(F32), 0.0).astype(BF16)
    tall = jnp.concatenate([owned] * (DK // QUARTER), axis=0)
    read[...] = jnp.sum(dot1(picked, tall), axis=0, keepdims=True)


def owner_rows(keep, got, query):
    return pl.pallas_call(
        owner_kernel,
        in_specs=[VMEM] * 3,
        out_specs=[VMEM] * 2,
        out_shape=[jax.ShapeDtypeStruct((QUARTER, DV), BF16), jax.ShapeDtypeStruct((1, DV), F32)],
        compiler_params=granted(4),
    )(keep, got, query)


def shards(
    layer_input,
    w_key,
    w_value,
    w_gates,
    decay_rate,
    beta_bias,
    log_decay_extra,
    new_query,
    read_gain,
):
    prompts, _, _ = layer_input.shape
    sp = lax.axis_size("sp")
    tp = lax.axis_size("tp")
    chunks = sp // prompts
    place = lax.axis_index("sp")
    pair = [(i, i ^ 1) for i in range(tp)]
    picked = jnp.where(place % 2 == 1, w_value, w_key)
    first = lax.ppermute(picked, "tp", pair)
    second = lax.ppermute(first, "sp", [(i, i ^ 1) for i in range(sp)])

    sent = packed(layer_input, log_decay_extra[:, 0, :])
    groups = [[prompts * t + j for j in range(prompts)] for t in range(chunks)]
    here = lax.all_to_all(sent, "sp", 0, 0, axis_index_groups=groups, tiled=True)

    parcel = parcels(here, decay_rate, beta_bias, tp)
    gathered = lax.all_to_all(parcel, "tp", 0, 0, tiled=True)

    gate_rows = w_gates.transpose(0, 2, 1).reshape(2 * tp, -1)
    used = gathered.shape[1] - PAD
    gate_shape = jax.ShapeDtypeStruct((gate_rows.shape[0], used), F32)
    held = [pltpu.VMEM((2, *w_key.shape), BF16), pltpu.SemaphoreType.DMA((2,))]
    theirs, gates = head_call(
        partner_kernel,
        [gate_shape],
        held,
        used,
        [VMEM, HBM, HBM, VMEM],
        *(gathered, first, second, gate_rows),
    )
    other = lax.ppermute(theirs, "tp", pair)
    (mine,) = head_call(own_kernel, [], [], used, [VMEM] * 4, gathered, w_key, w_value, gates)
    whole = pair_composed(mine, other)

    ways = [
        (prompts * t + i, chunks * ((2 * t + SHIFT + i) % prompts) + t)
        for t in range(chunks)
        for i in range(prompts)
    ]
    moved = lax.ppermute(whole, "sp", ways)
    near = lax.ppermute(moved, "sp", [(i, i ^ 1) for i in range(sp)])
    keep, give = coupled(moved, near)
    got = lax.ppermute(give, "sp", [(i, i ^ 2) for i in range(sp)])
    state_cache, partial = owner_rows(keep, got, new_query)

    parts = lax.all_to_all(
        jnp.broadcast_to(partial[None], (sp, 1, DV)), "sp", 0, 0, tiled=True
    )
    raw = parts.reshape(prompts, chunks, DV).sum(axis=1)
    scaled = raw * lax.rsqrt(jnp.mean(raw * raw, axis=-1, keepdims=True) + EPS) * read_gain
    return state_cache, scaled.astype(BF16)


def solution(mesh):
    placed = (
        P(None, "sp", "tp"),
        P(None, "tp"),
        P(None, "tp"),
        P(),
        P("tp"),
        P("tp"),
        P(None, "tp", "sp"),
        P(None, "tp"),
        P(),
    )

    return jax.shard_map(
        shards, mesh=mesh, in_specs=placed, out_specs=(P("sp", "tp"), P(None, "tp")), check_vma=False
    )
```

```python
import jax
import jax.numpy as jnp
from jax import lax
from jax.experimental import pallas as pl
from jax.experimental.pallas import tpu as pltpu
from jax.sharding import PartitionSpec as P


DK = 128
DV = 128
BLOCK = 128
EPS = 1e-06
HIGH = lax.Precision.HIGHEST
F32 = jnp.float32
BF16 = jnp.bfloat16
PAD = 16
GRANT = 24
SHIFT = 5


MIB = 1 << 20
VMEM = pl.BlockSpec(memory_space=pltpu.VMEM)
SMEM = pl.BlockSpec(memory_space=pltpu.SMEM)
HBM = pl.BlockSpec(memory_space=pltpu.HBM)


def granted(mib):
    return pltpu.CompilerParams(vmem_limit_bytes=mib * MIB)


NN = (((1,), (0,)), ((), ()))
NT = (((1,), (1,)), ((), ()))


def dot1(left, right, dims=NN):
    return lax.dot_general(left, right, dims, preferred_element_type=F32)


def halves(x):
    high = x.astype(BF16)
    low = (x - high.astype(F32)).astype(BF16)
    return high, low


def dot3(left, right, dims=NN):
    (la,), (ra,) = dims[0]
    lh, ll = halves(left)
    rh, rl = halves(right)
    return dot1(
        jnp.concatenate([lh, ll, lh], axis=la), jnp.concatenate([rh, rh, rl], axis=ra), dims
    )


MIB = 1 << 20
VMEM = pl.BlockSpec(memory_space=pltpu.VMEM)
SMEM = pl.BlockSpec(memory_space=pltpu.SMEM)
HBM = pl.BlockSpec(memory_space=pltpu.HBM)


def granted(mib):
    return pltpu.CompilerParams(vmem_limit_bytes=mib * MIB)


NN = (((1,), (0,)), ((), ()))
NT = (((1,), (1,)), ((), ()))


def dot1(left, right, dims=NN):
    return lax.dot_general(left, right, dims, preferred_element_type=F32)


def halves(x):
    high = x.astype(BF16)
    low = (x - high.astype(F32)).astype(BF16)
    return high, low


def dot3(left, right, dims=NN):
    (la,), (ra,) = dims[0]
    lh, ll = halves(left)
    rh, rl = halves(right)
    return dot1(
        jnp.concatenate([lh, ll, lh], axis=la), jnp.concatenate([rh, rh, rl], axis=ra), dims
    )


def three_pieces(x):
    high = x.astype(BF16).astype(F32)
    rest = x - high
    mid = rest.astype(BF16).astype(F32)
    return high, mid, (rest - mid).astype(BF16).astype(F32)


def pack_kernel(x, extra, out, held, sem):
    prompts, seg, width = x.shape
    first = lax.axis_index("sp") // prompts * 2 + SHIFT
    which = lambda i: lax.rem(first + i, prompts)
    copies = [
        pltpu.make_async_copy(x.at[which(i)], out.at[i, pl.ds(0, seg)], sem.at[i])
        for i in range(prompts)
    ]
    copies.append(pltpu.make_async_copy(extra, held, sem.at[prompts]))
    for copy in reversed(copies):
        copy.start()
    copies[-1].wait()
    for i in range(prompts):
        rows = list(three_pieces(held[pl.ds(which(i), 1), :])) + [jnp.zeros((PAD - 3, width), F32)]
        out[i, seg:, :] = jnp.concatenate(rows, axis=0).astype(BF16)
    for copy in copies[:-1]:
        copy.wait()


def packed(layer_input, extra):
    prompts, seg, width = layer_input.shape
    return pl.pallas_call(
        pack_kernel,
        in_specs=[HBM, HBM],
        out_specs=VMEM,
        out_shape=jax.ShapeDtypeStruct((prompts, seg + PAD, width), BF16),
        scratch_shapes=[pltpu.VMEM(extra.shape, F32), pltpu.SemaphoreType.DMA((prompts + 1,))],
        compiler_params=granted(60),
    )(layer_input, extra)


def parcel_kernel(here, rate, bias, out):
    segs, rows, width = here.shape
    seg = rows - PAD
    half = segs // 2
    lane = lax.broadcasted_iota(jnp.int32, (1, width), 1)
    consts = three_pieces(jnp.where(lane < width // 2, rate[0], bias[0]))
    for which in range(2):
        tails = [here[half * which + b, seg:, :].astype(F32) for b in range(half)]
        tail = [tails[b][i : i + 1] for i in range(3) for b in range(half)]
        tail = jnp.concatenate(tail + list(consts) + [jnp.zeros((PAD - 3 * half - 3, width), F32)], axis=0)
        tail = tail.astype(BF16)
        body = [here[half * which + b, :seg, :] for b in range(half)]
        for other in range(which, out.shape[0], 2):
            for b in range(half):
                out[other, seg * b : seg * (b + 1), :] = body[b]
            out[other, seg * half :, :] = tail


def parcels(here, rate, bias, count):
    segs, rows, width = here.shape
    return pl.pallas_call(
        parcel_kernel,
        in_specs=[VMEM, SMEM, SMEM],
        out_specs=VMEM,
        out_shape=jax.ShapeDtypeStruct((count, (segs // 2) * (rows - PAD) + PAD, width), BF16),
        compiler_params=granted(8),
    )(here, rate, bias)


def invert_unit_lower(units, row, col):
    size = BLOCK
    step = 1
    while step < size:
        merge = ((row // (2 * step)) == (col // (2 * step))) & ((row // step) != (col // step))
        if step == 1:
            eye = (row == col).astype(F32)
            for low, inverse, _, u in units:
                part = jnp.where(merge, low[u].astype(F32), 0.0)
                inverse[u] = (eye - part).astype(BF16)
        else:
            if step < 16:
                lower_rows = [(0, size)]
            else:
                lower_rows = [(at, step) for at in range(step, size, 2 * step)]
            rows = sum(length for _, length in lower_rows)
            take = lambda ref, u: jnp.concatenate([ref[u, at : at + n, :] for at, n in lower_rows], axis=0)
            for low, inverse, product, u in units:
                part = jnp.where(merge, low[u].astype(F32), 0.0).astype(BF16)
                product[u, :rows, :] = dot1(take(inverse, u), part).astype(BF16)
            for _, inverse, product, u in units:
                fill = dot1(product[u, :rows, :], inverse[u])
                fill = (take(inverse, u).astype(F32) - fill).astype(BF16)
                done = 0
                for at, n in lower_rows:
                    inverse[u, at : at + n, :] = fill[done : done + n]
                    done += n
        step *= 2


def squares():
    row = lax.broadcasted_iota(jnp.int32, (BLOCK, BLOCK), 0)
    return row, lax.broadcasted_iota(jnp.int32, (BLOCK, BLOCK), 1)


def first_kernel(xg, wk, wv, first, second, wg, out, *refs):
    own, refs = refs[:6], refs[6:]
    theirs, (acc, gates, product, solved, maps, weights, sem) = refs[:6], refs[6:]
    core = lax.axis_index("sp") % 2
    copies = [
        pltpu.make_async_copy(first, weights.at[core], sem.at[0]),
        pltpu.make_async_copy(second, weights.at[1 - core], sem.at[1]),
    ]
    for copy in copies:
        copy.start()
    sources, rows, width = xg.shape
    rows = rows - PAD
    blocks = rows // BLOCK
    x = jnp.concatenate([xg[i, :rows, :] for i in range(sources)], axis=1)
    gates[...] = dot1(wg[...], x, NT)
    acc[0] = dot1(x, jnp.concatenate([wk[...], wv[...]], axis=1))
    for copy in copies:
        copy.wait()
    acc[1] = dot1(x, jnp.concatenate([weights[0], weights[1]], axis=1))

    row, col = squares()
    strict = row > col
    upto = (row <= col).astype(F32)
    me = lax.axis_index("tp")
    cut = lambda g: jnp.concatenate([g[:, BLOCK * b : BLOCK * (b + 1)] for b in range(blocks)], axis=0)
    decays, betas = [], []
    for head in (me, me ^ 1):
        extras = xg[head, rows:, :].astype(F32)
        extra = extras[0:4] + extras[4:8] + extras[8:12]
        consts = extras[12:13] + extras[13:14] + extras[14:15]
        rate, bias = consts[:, 0:1], consts[:, width // 2 : width // 2 + 1]
        decay_pre = cut(gates[pl.ds(head, 1), :])
        beta_pre = cut(gates[pl.ds(sources + head, 1), :])
        soft = jnp.maximum(decay_pre, 0.0) + jnp.log1p(jnp.exp(-jnp.abs(decay_pre)))
        decays.append(-rate * soft + extra)
        betas.append(jax.nn.sigmoid(beta_pre + bias))
    running = jnp.dot(jnp.concatenate(decays, axis=0), upto, precision=HIGH, preferred_element_type=F32)
    count = 2 * blocks
    fill = jnp.zeros((BLOCK - 2 * count, BLOCK), F32)
    columns = jnp.concatenate([running, jnp.concatenate(betas, axis=0), fill], axis=0).T
    run_col = lambda u: jnp.broadcast_to(columns[:, u : u + 1], (BLOCK, BLOCK))
    beta_col = lambda u: jnp.broadcast_to(columns[:, count + u : count + u + 1], (BLOCK, BLOCK))
    last = lambda u: jnp.broadcast_to(running[u : u + 1, BLOCK - 1 :], (1, BLOCK))
    units = [(refs, which * blocks + b, b) for which, refs in enumerate((own, theirs)) for b in range(blocks)]
    for (late, low, rest, inverse, right, total), u, b in units:
        which = u // blocks
        pre = acc[which, BLOCK * b : BLOCK * (b + 1), :]
        act = pre * jax.nn.sigmoid(pre)
        key, value = act[:, :DK], act[:, DK:]
        key = key * lax.rsqrt(jnp.sum(key * key, axis=1, keepdims=True) + EPS)
        late[b] = key
        right[b, :, :DK] = key * (beta_col(u) * jnp.exp(run_col(u)))
        right[b, :, DK:] = value * beta_col(u)
        total[b : b + 1, :] = jnp.exp(last(u))
    for (late, low, rest, inverse, right, total), u, b in units:
        key = late[b]
        gram = dot3(key, key, NT)
        run_row = jnp.broadcast_to(running[u : u + 1, :], (BLOCK, BLOCK))
        weight = jnp.exp(jnp.where(strict, run_col(u) - run_row, 0.0))
        high, lower = halves(jnp.where(strict, gram * beta_col(u) * weight, 0.0))
        low[b] = high
        rest[b] = lower
        late[b] = key * jnp.exp(jnp.broadcast_to(last(u), (BLOCK, BLOCK)) - run_col(u))
    invert_unit_lower(
        [(refs[1], refs[3], product.at[u // blocks], b) for refs, u, b in units], row, col
    )
    finish(theirs, out, solved, maps)


def second_kernel(late, low, rest, inverse, right, total, out, solved, maps, held):
    held[...] = right[...]
    finish((late, low, rest, inverse, held, total), out, solved, maps)


def finish(refs, out, solved, maps):
    late, low, rest, inverse, right, total = refs
    row, col = squares()
    blocks = maps.shape[0]
    for u in range(blocks):
        solved[u] = dot1(inverse[u], right[u].astype(BF16)).astype(BF16)
    for u in range(blocks):
        first = solved[u]
        taken = dot1(jnp.concatenate([low[u], rest[u]], axis=1), jnp.concatenate([first, first], axis=0))
        right[u] = right[u] - first.astype(F32) - taken
    for u in range(blocks):
        right[u] = solved[u].astype(F32) + dot1(inverse[u], right[u].astype(BF16))
    for u in range(blocks):
        made = dot3(late[u].T, right[u])
        keep = jnp.where(row == col, jnp.broadcast_to(total[u : u + 1, :], (BLOCK, BLOCK)), 0.0)
        maps[u, :, :DK] = keep - made[:, :DK]
        maps[u, :, DK:] = made[:, DK:]
    apart = 1
    while apart < blocks:
        for u in range(0, blocks, 2 * apart):
            result = composed(maps[u], maps[u + apart])
            if 2 * apart < blocks:
                maps[u] = result
            else:
                out[...] = result
        apart *= 2


def composed(earlier, later):
    both = dot3(later[:, :DK], earlier)
    return jnp.concatenate([both[:, :DK], both[:, DK:] + later[:, DK:]], axis=1)


MAP = jax.ShapeDtypeStruct((DK, DK + DV), F32)


def block_arrays(blocks):
    wide, square = (blocks, BLOCK, DK + DV), (blocks, BLOCK, BLOCK)
    return [(square, F32), (square, BF16), (square, BF16), (square, BF16), (wide, F32), ((8, BLOCK), F32)]


def map_scratch(blocks):
    return [pltpu.VMEM((blocks, BLOCK, DK + DV), BF16), pltpu.VMEM((blocks, DK, DK + DV), F32)]


def partner_map(xg, w_key, w_value, first, second, gate_rows):
    used = xg.shape[1] - PAD
    blocks = used // BLOCK
    kept = block_arrays(blocks)
    return pl.pallas_call(
        first_kernel,
        in_specs=[VMEM, VMEM, VMEM, HBM, HBM, VMEM],
        out_specs=[VMEM] * (1 + len(kept)),
        out_shape=[MAP] + [jax.ShapeDtypeStruct(*a) for a in kept],
        scratch_shapes=[
            *[pltpu.VMEM(*a) for a in kept],
            pltpu.VMEM((2, used, DK + DV), F32),
            pltpu.VMEM((gate_rows.shape[0], used), F32),
            pltpu.VMEM((2, blocks, BLOCK, BLOCK), BF16),
            *map_scratch(blocks),
            pltpu.VMEM((2, *w_key.shape), BF16),
            pltpu.SemaphoreType.DMA((2,)),
        ],
        compiler_params=granted(GRANT),
    )(xg, w_key, w_value, first, second, gate_rows)


def own_map(*arrays):
    blocks = arrays[0].shape[0]
    return pl.pallas_call(
        second_kernel,
        in_specs=[VMEM] * len(arrays),
        out_specs=VMEM,
        out_shape=MAP,
        scratch_shapes=[*map_scratch(blocks), pltpu.VMEM((blocks, BLOCK, DK + DV), F32)],
        compiler_params=granted(8),
    )(*arrays)


def in_order(mine, other, late):
    earlier = jnp.where(late, other, mine)
    later = jnp.where(late, mine, other)
    return composed(earlier, later)


def diagonal():
    row = lax.broadcasted_iota(jnp.int32, (DK, DK), 0)
    return row == lax.broadcasted_iota(jnp.int32, (DK, DK), 1)


def pair_kernel(mine, other, out):
    whole = in_order(mine[...], other[...], lax.axis_index("tp") % 2 == 1)
    out[:DK, :] = whole.astype(BF16)
    part = whole[:, :DK]
    lost = part - part.astype(BF16).astype(F32)
    lost = jnp.sum(jnp.where(diagonal(), lost, 0.0), axis=0, keepdims=True)
    lost = jnp.concatenate([lost, jnp.zeros((PAD - 1, DK), F32)], axis=0)
    out[DK:, :] = jnp.concatenate([lost, jnp.zeros_like(lost)], axis=1).astype(BF16)


def widened(sent):
    whole = sent[:DK, :].astype(F32)
    lost = sent[DK:, :DK].astype(F32)[:1]
    part = whole[:, :DK] + jnp.where(diagonal(), jnp.broadcast_to(lost, (DK, DK)), 0.0)
    return jnp.concatenate([part, whole[:, DK:]], axis=1)


def pair_composed(mine, other):
    return pl.pallas_call(
        pair_kernel,
        in_specs=[VMEM] * 2,
        out_specs=VMEM,
        out_shape=jax.ShapeDtypeStruct((DK + PAD, DK + DV), BF16),
        compiler_params=granted(4),
    )(mine, other)


QUARTER = 32


def couple_kernel(mine, other, keep, give):
    place = lax.axis_index("sp")
    whole = in_order(widened(mine[...]), widened(other[...]), place % 2 == 1)
    keep[...] = whole
    core = place % 2

    @pl.when((place // 2) % 2 == 0)
    def _():
        give[...] = whole[:, DK:]

    @pl.when((place // 2) % 2 == 1)
    def _():
        mine_rows = pl.ds(pl.multiple_of(core * QUARTER, QUARTER), QUARTER)
        give[0:QUARTER, :] = keep[mine_rows, :DK]
        give[QUARTER : 2 * QUARTER, :] = keep[mine_rows, DK:]
        give[2 * QUARTER :, :] = jnp.zeros((DK - 2 * QUARTER, DV), F32)


def coupled(mine, other):
    return pl.pallas_call(
        couple_kernel,
        in_specs=[VMEM] * 2,
        out_specs=[VMEM] * 2,
        out_shape=[jax.ShapeDtypeStruct((DK, DK + DV), F32), jax.ShapeDtypeStruct((DK, DV), F32)],
        compiler_params=granted(4),
    )(mine, other)


def owner_kernel(keep, got, query, state, read):
    place = lax.axis_index("sp")
    late = (place // 2) % 2 == 1
    core = place % 2
    rows = pl.ds(pl.multiple_of(2 * QUARTER + core * QUARTER, QUARTER), QUARTER)
    early = jnp.where(late, got[...], keep[:, DK:])
    last_map = jnp.where(late, keep[rows, :DK], got[0:QUARTER, :])
    last_add = jnp.where(late, keep[rows, DK:], got[QUARTER : 2 * QUARTER, :])
    owned = (dot3(last_map, early) + last_add).astype(BF16)
    state[...] = owned
    which = lax.broadcasted_iota(jnp.int32, query.shape, 0)
    lane = lax.broadcasted_iota(jnp.int32, query.shape, 1)
    chosen = (which == place // 4) & (lane // QUARTER == place % 4)
    picked = jnp.where(chosen, query[...].astype(F32), 0.0).astype(BF16)
    tall = jnp.concatenate([owned] * (DK // QUARTER), axis=0)
    read[...] = jnp.sum(dot1(picked, tall), axis=0, keepdims=True)


def owner_rows(keep, got, query):
    return pl.pallas_call(
        owner_kernel,
        in_specs=[VMEM] * 3,
        out_specs=[VMEM] * 2,
        out_shape=[jax.ShapeDtypeStruct((QUARTER, DV), BF16), jax.ShapeDtypeStruct((1, DV), F32)],
        compiler_params=granted(4),
    )(keep, got, query)


def shards(
    layer_input,
    w_key,
    w_value,
    w_gates,
    decay_rate,
    beta_bias,
    log_decay_extra,
    new_query,
    read_gain,
):
    prompts, _, _ = layer_input.shape
    sp = lax.axis_size("sp")
    tp = lax.axis_size("tp")
    chunks = sp // prompts
    place = lax.axis_index("sp")
    pair = [(i, i ^ 1) for i in range(tp)]
    picked = jnp.where(place % 2 == 1, w_value, w_key)
    first = lax.ppermute(picked, "tp", pair)
    second = lax.ppermute(first, "sp", [(i, i ^ 1) for i in range(sp)])

    sent = packed(layer_input, log_decay_extra[:, 0, :])
    groups = [[prompts * t + j for j in range(prompts)] for t in range(chunks)]
    here = lax.all_to_all(sent, "sp", 0, 0, axis_index_groups=groups, tiled=True)

    parcel = parcels(here, decay_rate, beta_bias, tp)
    gathered = lax.all_to_all(parcel, "tp", 0, 0, tiled=True)

    gate_rows = w_gates.transpose(0, 2, 1).reshape(2 * tp, -1)
    theirs, *kept = partner_map(gathered, w_key, w_value, first, second, gate_rows)
    other = lax.ppermute(theirs, "tp", pair)
    mine = own_map(*kept)
    whole = pair_composed(mine, other)

    ways = [
        (prompts * t + i, chunks * ((2 * t + SHIFT + i) % prompts) + t)
        for t in range(chunks)
        for i in range(prompts)
    ]
    moved = lax.ppermute(whole, "sp", ways)
    near = lax.ppermute(moved, "sp", [(i, i ^ 1) for i in range(sp)])
    keep, give = coupled(moved, near)
    got = lax.ppermute(give, "sp", [(i, i ^ 2) for i in range(sp)])
    state_cache, partial = owner_rows(keep, got, new_query)

    parts = lax.all_to_all(
        jnp.broadcast_to(partial[None], (sp, 1, DV)), "sp", 0, 0, tiled=True
    )
    raw = parts.reshape(prompts, chunks, DV).sum(axis=1)
    scaled = raw * lax.rsqrt(jnp.mean(raw * raw, axis=-1, keepdims=True) + EPS) * read_gain
    return state_cache, scaled.astype(BF16)


def solution(mesh):
    placed = (
        P(None, "sp", "tp"),
        P(None, "tp"),
        P(None, "tp"),
        P(),
        P("tp"),
        P("tp"),
        P(None, "tp", "sp"),
        P(None, "tp"),
        P(),
    )

    return jax.shard_map(
        shards, mesh=mesh, in_specs=placed, out_specs=(P("sp", "tp"), P(None, "tp")), check_vma=False
    )
```

```python
import jax
import jax.numpy as jnp
from jax import lax
from jax.experimental import pallas as pl
from jax.experimental.pallas import tpu as pltpu
from jax.sharding import PartitionSpec as P


DK = 128
DV = 128
BLOCK = 128
EPS = 1e-06
HIGH = lax.Precision.HIGHEST
F32 = jnp.float32
BF16 = jnp.bfloat16
PAD = 16
SHIFT = 5


MIB = 1 << 20
VMEM = pl.BlockSpec(memory_space=pltpu.VMEM)
SMEM = pl.BlockSpec(memory_space=pltpu.SMEM)
HBM = pl.BlockSpec(memory_space=pltpu.HBM)


def granted(mib):
    return pltpu.CompilerParams(vmem_limit_bytes=mib * MIB)


NN = (((1,), (0,)), ((), ()))
NT = (((1,), (1,)), ((), ()))


def dot1(left, right, dims=NN):
    return lax.dot_general(left, right, dims, preferred_element_type=F32)


def halves(x):
    high = x.astype(BF16)
    low = (x - high.astype(F32)).astype(BF16)
    return high, low


def dot3(left, right, dims=NN):
    (la,), (ra,) = dims[0]
    lh, ll = halves(left)
    rh, rl = halves(right)
    return dot1(
        jnp.concatenate([lh, ll, lh], axis=la), jnp.concatenate([rh, rh, rl], axis=ra), dims
    )


MIB = 1 << 20
VMEM = pl.BlockSpec(memory_space=pltpu.VMEM)
SMEM = pl.BlockSpec(memory_space=pltpu.SMEM)
HBM = pl.BlockSpec(memory_space=pltpu.HBM)


def granted(mib):
    return pltpu.CompilerParams(vmem_limit_bytes=mib * MIB)


NN = (((1,), (0,)), ((), ()))
NT = (((1,), (1,)), ((), ()))


def dot1(left, right, dims=NN):
    return lax.dot_general(left, right, dims, preferred_element_type=F32)


def halves(x):
    high = x.astype(BF16)
    low = (x - high.astype(F32)).astype(BF16)
    return high, low


def dot3(left, right, dims=NN):
    (la,), (ra,) = dims[0]
    lh, ll = halves(left)
    rh, rl = halves(right)
    return dot1(
        jnp.concatenate([lh, ll, lh], axis=la), jnp.concatenate([rh, rh, rl], axis=ra), dims
    )


def three_pieces(x):
    high = x.astype(BF16).astype(F32)
    rest = x - high
    mid = rest.astype(BF16).astype(F32)
    return high, mid, (rest - mid).astype(BF16).astype(F32)


def pack_kernel(x, extra, out, held, sem):
    prompts, seg, width = x.shape
    first = lax.axis_index("sp") // prompts * 2 + SHIFT
    which = lambda i: lax.rem(first + i, prompts)
    copies = [
        pltpu.make_async_copy(x.at[which(i)], out.at[i, pl.ds(0, seg)], sem.at[i])
        for i in range(prompts)
    ]
    copies.append(pltpu.make_async_copy(extra, held, sem.at[prompts]))
    for copy in reversed(copies):
        copy.start()
    copies[-1].wait()
    for i in range(prompts):
        rows = list(three_pieces(held[pl.ds(which(i), 1), :])) + [jnp.zeros((PAD - 3, width), F32)]
        out[i, seg:, :] = jnp.concatenate(rows, axis=0).astype(BF16)
    for copy in copies[:-1]:
        copy.wait()


def packed(layer_input, extra):
    prompts, seg, width = layer_input.shape
    return pl.pallas_call(
        pack_kernel,
        in_specs=[HBM, HBM],
        out_specs=VMEM,
        out_shape=jax.ShapeDtypeStruct((prompts, seg + PAD, width), BF16),
        scratch_shapes=[pltpu.VMEM(extra.shape, F32), pltpu.SemaphoreType.DMA((prompts + 1,))],
        compiler_params=granted(60),
    )(layer_input, extra)


def parcel_kernel(here, rate, bias, out):
    segs, rows, width = here.shape
    seg = rows - PAD
    half = segs // 2
    lane = lax.broadcasted_iota(jnp.int32, (1, width), 1)
    consts = three_pieces(jnp.where(lane < width // 2, rate[0], bias[0]))
    for which in range(2):
        tails = [here[half * which + b, seg:, :].astype(F32) for b in range(half)]
        tail = [tails[b][i : i + 1] for i in range(3) for b in range(half)]
        tail = jnp.concatenate(tail + list(consts) + [jnp.zeros((PAD - 3 * half - 3, width), F32)], axis=0)
        tail = tail.astype(BF16)
        body = [here[half * which + b, :seg, :] for b in range(half)]
        for other in range(which, out.shape[0], 2):
            for b in range(half):
                out[other, seg * b : seg * (b + 1), :] = body[b]
            out[other, seg * half :, :] = tail


def parcels(here, rate, bias, count):
    segs, rows, width = here.shape
    return pl.pallas_call(
        parcel_kernel,
        in_specs=[VMEM, SMEM, SMEM],
        out_specs=VMEM,
        out_shape=jax.ShapeDtypeStruct((count, (segs // 2) * (rows - PAD) + PAD, width), BF16),
        compiler_params=granted(8),
    )(here, rate, bias)


def invert_unit_lower(low, inverse, product, row, col):
    units, size, _ = low.shape
    step = 1
    while step < size:
        merge = ((row // (2 * step)) == (col // (2 * step))) & ((row // step) != (col // step))
        if step == 1:
            eye = (row == col).astype(F32)
            for u in range(units):
                part = jnp.where(merge, low[u].astype(F32), 0.0)
                inverse[u] = (eye - part).astype(BF16)
        else:
            if step < 16:
                lower_rows = [(0, size)]
            else:
                lower_rows = [(at, step) for at in range(step, size, 2 * step)]
            rows = sum(length for _, length in lower_rows)
            take = lambda u: jnp.concatenate([inverse[u, at : at + n, :] for at, n in lower_rows], axis=0)
            for u in range(units):
                part = jnp.where(merge, low[u].astype(F32), 0.0).astype(BF16)
                product[u, :rows, :] = dot1(take(u), part).astype(BF16)
            for u in range(units):
                fill = dot1(product[u, :rows, :], inverse[u])
                fill = (take(u).astype(F32) - fill).astype(BF16)
                done = 0
                for at, n in lower_rows:
                    inverse[u, at : at + n, :] = fill[done : done + n]
                    done += n
        step *= 2


def gate_kernel(xg, wg, gates):
    gates[...] = dot1(wg[...], features(xg), NT)


def gate_sums(xg, gate_rows):
    return pl.pallas_call(
        gate_kernel,
        in_specs=[VMEM] * 2,
        out_specs=VMEM,
        out_shape=jax.ShapeDtypeStruct((gate_rows.shape[0], xg.shape[1] - PAD), F32),
        compiler_params=granted(8),
    )(xg, gate_rows)


def partner_kernel(xg, first, second, gates, out, *scratch):
    turned = lax.axis_index("sp") % 2 == 1
    w_key = jnp.where(turned, second[...], first[...])
    w_value = jnp.where(turned, first[...], second[...])
    head_map(lax.axis_index("tp") ^ 1, features(xg), xg, w_key, w_value, gates, out, *scratch)


def own_kernel(xg, w_key, w_value, gates, out, *scratch):
    head_map(lax.axis_index("tp"), features(xg), xg, w_key[...], w_value[...], gates, out, *scratch)


def features(xg):
    sources, rows, _ = xg.shape
    return jnp.concatenate([xg[i, : rows - PAD, :] for i in range(sources)], axis=1)


def head_map(head, x, xg, w_key, w_value, gates, out, acc, keys, low, low_rest, inverse, product, right, solved, maps):
    sources, rows, width = xg.shape
    rows = rows - PAD
    blocks = units = rows // BLOCK
    acc[...] = dot1(x, jnp.concatenate([w_key, w_value], axis=1))

    row = lax.broadcasted_iota(jnp.int32, (BLOCK, BLOCK), 0)
    col = lax.broadcasted_iota(jnp.int32, (BLOCK, BLOCK), 1)
    upto = (row <= col).astype(F32)
    strict = row > col
    extras = xg[head, rows:, :].astype(F32)
    extra = extras[0:4] + extras[4:8] + extras[8:12]
    consts = extras[12:13] + extras[13:14] + extras[14:15]
    rate, bias = consts[:, 0:1], consts[:, width // 2 : width // 2 + 1]
    cut = lambda g: jnp.concatenate([g[:, BLOCK * b : BLOCK * (b + 1)] for b in range(blocks)], axis=0)
    decay_pre = cut(gates[pl.ds(head, 1), :])
    beta_pre = cut(gates[pl.ds(sources + head, 1), :])
    soft = jnp.maximum(decay_pre, 0.0) + jnp.log1p(jnp.exp(-jnp.abs(decay_pre)))
    beta = jax.nn.sigmoid(beta_pre + bias)
    decay = jnp.concatenate([-rate * soft + extra, jnp.zeros((8 - blocks, BLOCK), F32)], axis=0)
    running = jnp.dot(decay, upto, precision=HIGH, preferred_element_type=F32)[:units]
    tall = jnp.concatenate([running, beta, jnp.zeros((BLOCK - 2 * units, BLOCK), F32)], axis=0)
    columns = tall.T
    run_col = lambda u: jnp.broadcast_to(columns[:, u : u + 1], (BLOCK, BLOCK))
    beta_col = lambda u: jnp.broadcast_to(columns[:, units + u : units + u + 1], (BLOCK, BLOCK))
    run_row = lambda u: jnp.broadcast_to(running[u : u + 1, :], (BLOCK, BLOCK))
    last = lambda u: jnp.broadcast_to(running[u : u + 1, BLOCK - 1 :], (BLOCK, BLOCK))
    for u in range(units):
        pre = acc[BLOCK * u : BLOCK * (u + 1), :]
        act = pre * jax.nn.sigmoid(pre)
        key, value = act[:, :DK], act[:, DK:]
        key = key * lax.rsqrt(jnp.sum(key * key, axis=1, keepdims=True) + EPS)
        keys[u] = key
        strength = beta_col(u)
        right[u, :, :DK] = key * (strength * jnp.exp(run_col(u)))
        right[u, :, DK:] = value * strength
    for u in range(units):
        key = keys[u]
        gram = dot3(key, key, NT)
        weights = jnp.exp(jnp.where(strict, run_col(u) - run_row(u), 0.0))
        high, rest = halves(jnp.where(strict, gram * beta_col(u) * weights, 0.0))
        low[u] = high
        low_rest[u] = rest
    invert_unit_lower(low, inverse, product, row, col)
    for u in range(units):
        solved[u] = dot1(inverse[u], right[u].astype(BF16)).astype(BF16)
    for u in range(units):
        first = solved[u]
        taken = dot1(
            jnp.concatenate([low[u], low_rest[u]], axis=1), jnp.concatenate([first, first], axis=0)
        )
        right[u] = right[u] - first.astype(F32) - taken
    for u in range(units):
        right[u] = solved[u].astype(F32) + dot1(inverse[u], right[u].astype(BF16))
    for u in range(units):
        late = keys[u] * jnp.exp(last(u) - run_col(u))
        made = dot3(late.T, right[u])
        keep = jnp.where(row == col, jnp.exp(last(u)), 0.0)
        maps[u, :, :DK] = keep - made[:, :DK]
        maps[u, :, DK:] = made[:, DK:]
    apart = 1
    while apart < blocks:
        for u in range(0, units, 2 * apart):
            result = composed(maps[u], maps[u + apart])
            if 2 * apart < blocks:
                maps[u] = result
            else:
                out[...] = result
        apart *= 2


def composed(earlier, later):
    both = dot3(later[:, :DK], earlier)
    return jnp.concatenate([both[:, :DK], both[:, DK:] + later[:, DK:]], axis=1)


def head_call(kernel, *operands):
    used = operands[0].shape[1] - PAD
    units = used // BLOCK
    return pl.pallas_call(
        kernel,
        in_specs=[VMEM] * len(operands),
        out_specs=VMEM,
        out_shape=jax.ShapeDtypeStruct((DK, DK + DV), F32),
        scratch_shapes=[
            pltpu.VMEM((used, DK + DV), F32),
            pltpu.VMEM((units, BLOCK, DK), F32),
            pltpu.VMEM((units, BLOCK, BLOCK), BF16),
            pltpu.VMEM((units, BLOCK, BLOCK), BF16),
            pltpu.VMEM((units, BLOCK, BLOCK), BF16),
            pltpu.VMEM((units, BLOCK, BLOCK), BF16),
            pltpu.VMEM((units, BLOCK, DK + DV), F32),
            pltpu.VMEM((units, BLOCK, DK + DV), BF16),
            pltpu.VMEM((units, DK, DK + DV), F32),
        ],
        compiler_params=granted(24),
    )(*operands)


def in_order(mine, other, late):
    earlier = jnp.where(late, other, mine)
    later = jnp.where(late, mine, other)
    return composed(earlier, later)


def diagonal():
    row = lax.broadcasted_iota(jnp.int32, (DK, DK), 0)
    return row == lax.broadcasted_iota(jnp.int32, (DK, DK), 1)


def pair_kernel(mine, other, out):
    whole = in_order(mine[...], other[...], lax.axis_index("tp") % 2 == 1)
    out[:DK, :] = whole.astype(BF16)
    part = whole[:, :DK]
    lost = part - part.astype(BF16).astype(F32)
    lost = jnp.sum(jnp.where(diagonal(), lost, 0.0), axis=0, keepdims=True)
    lost = jnp.concatenate([lost, jnp.zeros((PAD - 1, DK), F32)], axis=0)
    out[DK:, :] = jnp.concatenate([lost, jnp.zeros_like(lost)], axis=1).astype(BF16)


def widened(sent):
    whole = sent[:DK, :].astype(F32)
    lost = sent[DK:, :DK].astype(F32)[:1]
    part = whole[:, :DK] + jnp.where(diagonal(), jnp.broadcast_to(lost, (DK, DK)), 0.0)
    return jnp.concatenate([part, whole[:, DK:]], axis=1)


def pair_composed(mine, other):
    return pl.pallas_call(
        pair_kernel,
        in_specs=[VMEM] * 2,
        out_specs=VMEM,
        out_shape=jax.ShapeDtypeStruct((DK + PAD, DK + DV), BF16),
        compiler_params=granted(4),
    )(mine, other)


QUARTER = 32


def couple_kernel(mine, other, keep, give):
    place = lax.axis_index("sp")
    whole = in_order(widened(mine[...]), widened(other[...]), place % 2 == 1)
    keep[...] = whole
    core = place % 2

    @pl.when((place // 2) % 2 == 0)
    def _():
        give[...] = whole[:, DK:]

    @pl.when((place // 2) % 2 == 1)
    def _():
        mine_rows = pl.ds(pl.multiple_of(core * QUARTER, QUARTER), QUARTER)
        give[0:QUARTER, :] = keep[mine_rows, :DK]
        give[QUARTER : 2 * QUARTER, :] = keep[mine_rows, DK:]
        give[2 * QUARTER :, :] = jnp.zeros((DK - 2 * QUARTER, DV), F32)


def coupled(mine, other):
    return pl.pallas_call(
        couple_kernel,
        in_specs=[VMEM] * 2,
        out_specs=[VMEM] * 2,
        out_shape=[jax.ShapeDtypeStruct((DK, DK + DV), F32), jax.ShapeDtypeStruct((DK, DV), F32)],
        compiler_params=granted(4),
    )(mine, other)


def owner_kernel(keep, got, query, state, read):
    place = lax.axis_index("sp")
    late = (place // 2) % 2 == 1
    core = place % 2
    rows = pl.ds(pl.multiple_of(2 * QUARTER + core * QUARTER, QUARTER), QUARTER)
    early = jnp.where(late, got[...], keep[:, DK:])
    last_map = jnp.where(late, keep[rows, :DK], got[0:QUARTER, :])
    last_add = jnp.where(late, keep[rows, DK:], got[QUARTER : 2 * QUARTER, :])
    owned = (dot3(last_map, early) + last_add).astype(BF16)
    state[...] = owned
    which = lax.broadcasted_iota(jnp.int32, query.shape, 0)
    lane = lax.broadcasted_iota(jnp.int32, query.shape, 1)
    chosen = (which == place // 4) & (lane // QUARTER == place % 4)
    picked = jnp.where(chosen, query[...].astype(F32), 0.0).astype(BF16)
    tall = jnp.concatenate([owned] * (DK // QUARTER), axis=0)
    read[...] = jnp.sum(dot1(picked, tall), axis=0, keepdims=True)


def owner_rows(keep, got, query):
    return pl.pallas_call(
        owner_kernel,
        in_specs=[VMEM] * 3,
        out_specs=[VMEM] * 2,
        out_shape=[jax.ShapeDtypeStruct((QUARTER, DV), BF16), jax.ShapeDtypeStruct((1, DV), F32)],
        compiler_params=granted(4),
    )(keep, got, query)


def shards(
    layer_input,
    w_key,
    w_value,
    w_gates,
    decay_rate,
    beta_bias,
    log_decay_extra,
    new_query,
    read_gain,
):
    prompts, _, _ = layer_input.shape
    sp = lax.axis_size("sp")
    tp = lax.axis_size("tp")
    chunks = sp // prompts
    place = lax.axis_index("sp")
    pair = [(i, i ^ 1) for i in range(tp)]
    picked = jnp.where(place % 2 == 1, w_value, w_key)
    first = lax.ppermute(picked, "tp", pair)
    second = lax.ppermute(first, "sp", [(i, i ^ 1) for i in range(sp)])

    sent = packed(layer_input, log_decay_extra[:, 0, :])
    groups = [[prompts * t + j for j in range(prompts)] for t in range(chunks)]
    here = lax.all_to_all(sent, "sp", 0, 0, axis_index_groups=groups, tiled=True)

    parcel = parcels(here, decay_rate, beta_bias, tp)
    gathered = lax.all_to_all(parcel, "tp", 0, 0, tiled=True)

    gate_rows = w_gates.transpose(0, 2, 1).reshape(2 * tp, -1)
    gates = gate_sums(gathered, gate_rows)
    theirs = head_call(partner_kernel, gathered, first, second, gates)
    other = lax.ppermute(theirs, "tp", pair)
    mine = head_call(own_kernel, gathered, w_key, w_value, gates)
    whole = pair_composed(mine, other)

    ways = [
        (prompts * t + i, chunks * ((2 * t + SHIFT + i) % prompts) + t)
        for t in range(chunks)
        for i in range(prompts)
    ]
    moved = lax.ppermute(whole, "sp", ways)
    near = lax.ppermute(moved, "sp", [(i, i ^ 1) for i in range(sp)])
    keep, give = coupled(moved, near)
    got = lax.ppermute(give, "sp", [(i, i ^ 2) for i in range(sp)])
    state_cache, partial = owner_rows(keep, got, new_query)

    parts = lax.all_to_all(
        jnp.broadcast_to(partial[None], (sp, 1, DV)), "sp", 0, 0, tiled=True
    )
    raw = parts.reshape(prompts, chunks, DV).sum(axis=1)
    scaled = raw * lax.rsqrt(jnp.mean(raw * raw, axis=-1, keepdims=True) + EPS) * read_gain
    return state_cache, scaled.astype(BF16)


def solution(mesh):
    placed = (
        P(None, "sp", "tp"),
        P(None, "tp"),
        P(None, "tp"),
        P(),
        P("tp"),
        P("tp"),
        P(None, "tp", "sp"),
        P(None, "tp"),
        P(),
    )

    return jax.shard_map(
        shards, mesh=mesh, in_specs=placed, out_specs=(P("sp", "tp"), P(None, "tp")), check_vma=False
    )
```

```python
import jax
import jax.numpy as jnp
from jax import lax
from jax.experimental import pallas as pl
from jax.experimental.pallas import tpu as pltpu
from jax.sharding import PartitionSpec as P


DK = 128
DV = 128
BLOCK = 128
EPS = 1e-06
HIGH = lax.Precision.HIGHEST
F32 = jnp.float32
BF16 = jnp.bfloat16
PAD = 16
SHIFT = 5


MIB = 1 << 20
VMEM = pl.BlockSpec(memory_space=pltpu.VMEM)
SMEM = pl.BlockSpec(memory_space=pltpu.SMEM)
HBM = pl.BlockSpec(memory_space=pltpu.HBM)


def granted(mib):
    return pltpu.CompilerParams(vmem_limit_bytes=mib * MIB)


NN = (((1,), (0,)), ((), ()))
NT = (((1,), (1,)), ((), ()))


def dot1(left, right, dims=NN):
    return lax.dot_general(left, right, dims, preferred_element_type=F32)


def halves(x):
    high = x.astype(BF16)
    low = (x - high.astype(F32)).astype(BF16)
    return high, low


def dot3(left, right, dims=NN):
    (la,), (ra,) = dims[0]
    lh, ll = halves(left)
    rh, rl = halves(right)
    return dot1(
        jnp.concatenate([lh, ll, lh], axis=la), jnp.concatenate([rh, rh, rl], axis=ra), dims
    )


MIB = 1 << 20
VMEM = pl.BlockSpec(memory_space=pltpu.VMEM)
SMEM = pl.BlockSpec(memory_space=pltpu.SMEM)
HBM = pl.BlockSpec(memory_space=pltpu.HBM)


def granted(mib):
    return pltpu.CompilerParams(vmem_limit_bytes=mib * MIB)


NN = (((1,), (0,)), ((), ()))
NT = (((1,), (1,)), ((), ()))


def dot1(left, right, dims=NN):
    return lax.dot_general(left, right, dims, preferred_element_type=F32)


def halves(x):
    high = x.astype(BF16)
    low = (x - high.astype(F32)).astype(BF16)
    return high, low


def dot3(left, right, dims=NN):
    (la,), (ra,) = dims[0]
    lh, ll = halves(left)
    rh, rl = halves(right)
    return dot1(
        jnp.concatenate([lh, ll, lh], axis=la), jnp.concatenate([rh, rh, rl], axis=ra), dims
    )


def three_pieces(x):
    high = x.astype(BF16).astype(F32)
    rest = x - high
    mid = rest.astype(BF16).astype(F32)
    return high, mid, (rest - mid).astype(BF16).astype(F32)


def pack_kernel(x, extra, out, staged, held, arrive, leave):
    prompts, seg, width = x.shape
    first = lax.axis_index("sp") // prompts * 2 + SHIFT
    which = lambda i: lax.rem(first + i, prompts)
    extras = pltpu.make_async_copy(extra, held, arrive.at[prompts])
    extras.start()
    coming = [
        pltpu.make_async_copy(x.at[which(i)], staged.at[i, pl.ds(0, seg)], arrive.at[i])
        for i in range(prompts)
    ]
    for copy in coming:
        copy.start()
    extras.wait()
    for i in range(prompts):
        rows = list(three_pieces(held[pl.ds(which(i), 1), :])) + [jnp.zeros((PAD - 3, width), F32)]
        staged[i, seg:, :] = jnp.concatenate(rows, axis=0).astype(BF16)
    going = [pltpu.make_async_copy(staged.at[i], out.at[i], leave.at[i]) for i in range(prompts)]
    for came, go in zip(coming, going):
        came.wait()
        go.start()
    for go in going:
        go.wait()


def packed(layer_input, extra):
    prompts, seg, width = layer_input.shape
    shape = (prompts, seg + PAD, width)
    return pl.pallas_call(
        pack_kernel,
        in_specs=[HBM, HBM],
        out_specs=HBM,
        out_shape=jax.ShapeDtypeStruct(shape, BF16),
        scratch_shapes=[
            pltpu.VMEM(shape, BF16),
            pltpu.VMEM(extra.shape, F32),
            pltpu.SemaphoreType.DMA((prompts + 1,)),
            pltpu.SemaphoreType.DMA((prompts,)),
        ],
        compiler_params=granted(60),
    )(layer_input, extra)


def parcel_kernel(here, rate, bias, out):
    segs, rows, width = here.shape
    seg = rows - PAD
    half = segs // 2
    lane = lax.broadcasted_iota(jnp.int32, (1, width), 1)
    consts = three_pieces(jnp.where(lane < width // 2, rate[0], bias[0]))
    for which in range(2):
        tails = [here[half * which + b, seg:, :].astype(F32) for b in range(half)]
        tail = [tails[b][i : i + 1] for i in range(3) for b in range(half)]
        tail = jnp.concatenate(tail + list(consts) + [jnp.zeros((PAD - 3 * half - 3, width), F32)], axis=0)
        tail = tail.astype(BF16)
        body = [here[half * which + b, :seg, :] for b in range(half)]
        for other in range(which, out.shape[0], 2):
            for b in range(half):
                out[other, seg * b : seg * (b + 1), :] = body[b]
            out[other, seg * half :, :] = tail


def parcels(here, rate, bias, count):
    segs, rows, width = here.shape
    return pl.pallas_call(
        parcel_kernel,
        in_specs=[VMEM, SMEM, SMEM],
        out_specs=VMEM,
        out_shape=jax.ShapeDtypeStruct((count, (segs // 2) * (rows - PAD) + PAD, width), BF16),
        compiler_params=granted(8),
    )(here, rate, bias)


def invert_unit_lower(low, inverse, product, row, col):
    units, size, _ = low.shape
    step = 1
    while step < size:
        merge = ((row // (2 * step)) == (col // (2 * step))) & ((row // step) != (col // step))
        if step == 1:
            eye = (row == col).astype(F32)
            for u in range(units):
                part = jnp.where(merge, low[u].astype(F32), 0.0)
                inverse[u] = (eye - part).astype(BF16)
        else:
            if step < 16:
                lower_rows = [(0, size)]
            else:
                lower_rows = [(at, step) for at in range(step, size, 2 * step)]
            rows = sum(length for _, length in lower_rows)
            take = lambda u: jnp.concatenate([inverse[u, at : at + n, :] for at, n in lower_rows], axis=0)
            for u in range(units):
                part = jnp.where(merge, low[u].astype(F32), 0.0).astype(BF16)
                product[u, :rows, :] = dot1(take(u), part).astype(BF16)
            for u in range(units):
                fill = dot1(product[u, :rows, :], inverse[u])
                fill = (take(u).astype(F32) - fill).astype(BF16)
                done = 0
                for at, n in lower_rows:
                    inverse[u, at : at + n, :] = fill[done : done + n]
                    done += n
        step *= 2


def gate_kernel(xg, wg, gates):
    gates[...] = dot1(wg[...], features(xg), NT)


def gate_sums(xg, gate_rows):
    return pl.pallas_call(
        gate_kernel,
        in_specs=[VMEM] * 2,
        out_specs=VMEM,
        out_shape=jax.ShapeDtypeStruct((gate_rows.shape[0], xg.shape[1] - PAD), F32),
        compiler_params=granted(8),
    )(xg, gate_rows)


def partner_kernel(xg, first, second, gates, out, *scratch):
    turned = lax.axis_index("sp") % 2 == 1
    w_key = jnp.where(turned, second[...], first[...])
    w_value = jnp.where(turned, first[...], second[...])
    head_map(lax.axis_index("tp") ^ 1, features(xg), xg, w_key, w_value, gates, out, *scratch)


def own_kernel(xg, w_key, w_value, gates, out, *scratch):
    head_map(lax.axis_index("tp"), features(xg), xg, w_key[...], w_value[...], gates, out, *scratch)


def features(xg):
    sources, rows, _ = xg.shape
    return jnp.concatenate([xg[i, : rows - PAD, :] for i in range(sources)], axis=1)


def head_map(head, x, xg, w_key, w_value, gates, out, acc, keys, low, low_rest, inverse, product, right, solved, maps):
    sources, rows, width = xg.shape
    rows = rows - PAD
    blocks = units = rows // BLOCK
    acc[...] = dot1(x, jnp.concatenate([w_key, w_value], axis=1))

    row = lax.broadcasted_iota(jnp.int32, (BLOCK, BLOCK), 0)
    col = lax.broadcasted_iota(jnp.int32, (BLOCK, BLOCK), 1)
    upto = (row <= col).astype(F32)
    strict = row > col
    extras = xg[head, rows:, :].astype(F32)
    extra = extras[0:4] + extras[4:8] + extras[8:12]
    consts = extras[12:13] + extras[13:14] + extras[14:15]
    rate, bias = consts[:, 0:1], consts[:, width // 2 : width // 2 + 1]
    cut = lambda g: jnp.concatenate([g[:, BLOCK * b : BLOCK * (b + 1)] for b in range(blocks)], axis=0)
    decay_pre = cut(gates[pl.ds(head, 1), :])
    beta_pre = cut(gates[pl.ds(sources + head, 1), :])
    soft = jnp.maximum(decay_pre, 0.0) + jnp.log1p(jnp.exp(-jnp.abs(decay_pre)))
    beta = jax.nn.sigmoid(beta_pre + bias)
    decay = jnp.concatenate([-rate * soft + extra, jnp.zeros((8 - blocks, BLOCK), F32)], axis=0)
    running = jnp.dot(decay, upto, precision=HIGH, preferred_element_type=F32)[:units]
    tall = jnp.concatenate([running, beta, jnp.zeros((BLOCK - 2 * units, BLOCK), F32)], axis=0)
    columns = tall.T
    run_col = lambda u: jnp.broadcast_to(columns[:, u : u + 1], (BLOCK, BLOCK))
    beta_col = lambda u: jnp.broadcast_to(columns[:, units + u : units + u + 1], (BLOCK, BLOCK))
    run_row = lambda u: jnp.broadcast_to(running[u : u + 1, :], (BLOCK, BLOCK))
    last = lambda u: jnp.broadcast_to(running[u : u + 1, BLOCK - 1 :], (BLOCK, BLOCK))
    for u in range(units):
        pre = acc[BLOCK * u : BLOCK * (u + 1), :]
        act = pre * jax.nn.sigmoid(pre)
        key, value = act[:, :DK], act[:, DK:]
        key = key * lax.rsqrt(jnp.sum(key * key, axis=1, keepdims=True) + EPS)
        keys[u] = key
        strength = beta_col(u)
        right[u, :, :DK] = key * (strength * jnp.exp(run_col(u)))
        right[u, :, DK:] = value * strength
    for u in range(units):
        key = keys[u]
        gram = dot3(key, key, NT)
        weights = jnp.exp(jnp.where(strict, run_col(u) - run_row(u), 0.0))
        high, rest = halves(jnp.where(strict, gram * beta_col(u) * weights, 0.0))
        low[u] = high
        low_rest[u] = rest
    invert_unit_lower(low, inverse, product, row, col)
    for u in range(units):
        solved[u] = dot1(inverse[u], right[u].astype(BF16)).astype(BF16)
    for u in range(units):
        first = solved[u]
        taken = dot1(
            jnp.concatenate([low[u], low_rest[u]], axis=1), jnp.concatenate([first, first], axis=0)
        )
        right[u] = right[u] - first.astype(F32) - taken
    for u in range(units):
        right[u] = solved[u].astype(F32) + dot1(inverse[u], right[u].astype(BF16))
    for u in range(units):
        late = keys[u] * jnp.exp(last(u) - run_col(u))
        made = dot3(late.T, right[u])
        keep = jnp.where(row == col, jnp.exp(last(u)), 0.0)
        maps[u, :, :DK] = keep - made[:, :DK]
        maps[u, :, DK:] = made[:, DK:]
    apart = 1
    while apart < blocks:
        for u in range(0, units, 2 * apart):
            result = composed(maps[u], maps[u + apart])
            if 2 * apart < blocks:
                maps[u] = result
            else:
                out[...] = result
        apart *= 2


def composed(earlier, later):
    both = dot3(later[:, :DK], earlier)
    return jnp.concatenate([both[:, :DK], both[:, DK:] + later[:, DK:]], axis=1)


def head_call(kernel, *operands):
    used = operands[0].shape[1] - PAD
    units = used // BLOCK
    return pl.pallas_call(
        kernel,
        in_specs=[VMEM] * len(operands),
        out_specs=VMEM,
        out_shape=jax.ShapeDtypeStruct((DK, DK + DV), F32),
        scratch_shapes=[
            pltpu.VMEM((used, DK + DV), F32),
            pltpu.VMEM((units, BLOCK, DK), F32),
            pltpu.VMEM((units, BLOCK, BLOCK), BF16),
            pltpu.VMEM((units, BLOCK, BLOCK), BF16),
            pltpu.VMEM((units, BLOCK, BLOCK), BF16),
            pltpu.VMEM((units, BLOCK, BLOCK), BF16),
            pltpu.VMEM((units, BLOCK, DK + DV), F32),
            pltpu.VMEM((units, BLOCK, DK + DV), BF16),
            pltpu.VMEM((units, DK, DK + DV), F32),
        ],
        compiler_params=granted(24),
    )(*operands)


def in_order(mine, other, late):
    earlier = jnp.where(late, other, mine)
    later = jnp.where(late, mine, other)
    return composed(earlier, later)


def diagonal():
    row = lax.broadcasted_iota(jnp.int32, (DK, DK), 0)
    return row == lax.broadcasted_iota(jnp.int32, (DK, DK), 1)


def pair_kernel(mine, other, out):
    whole = in_order(mine[...], other[...], lax.axis_index("tp") % 2 == 1)
    out[:DK, :] = whole.astype(BF16)
    part = whole[:, :DK]
    lost = part - part.astype(BF16).astype(F32)
    lost = jnp.sum(jnp.where(diagonal(), lost, 0.0), axis=0, keepdims=True)
    lost = jnp.concatenate([lost, jnp.zeros((PAD - 1, DK), F32)], axis=0)
    out[DK:, :] = jnp.concatenate([lost, jnp.zeros_like(lost)], axis=1).astype(BF16)


def widened(sent):
    whole = sent[:DK, :].astype(F32)
    lost = sent[DK:, :DK].astype(F32)[:1]
    part = whole[:, :DK] + jnp.where(diagonal(), jnp.broadcast_to(lost, (DK, DK)), 0.0)
    return jnp.concatenate([part, whole[:, DK:]], axis=1)


def pair_composed(mine, other):
    return pl.pallas_call(
        pair_kernel,
        in_specs=[VMEM] * 2,
        out_specs=VMEM,
        out_shape=jax.ShapeDtypeStruct((DK + PAD, DK + DV), BF16),
        compiler_params=granted(4),
    )(mine, other)


QUARTER = 32


def couple_kernel(mine, other, keep, give):
    place = lax.axis_index("sp")
    whole = in_order(widened(mine[...]), widened(other[...]), place % 2 == 1)
    keep[...] = whole
    core = place % 2

    @pl.when((place // 2) % 2 == 0)
    def _():
        give[...] = whole[:, DK:]

    @pl.when((place // 2) % 2 == 1)
    def _():
        mine_rows = pl.ds(pl.multiple_of(core * QUARTER, QUARTER), QUARTER)
        give[0:QUARTER, :] = keep[mine_rows, :DK]
        give[QUARTER : 2 * QUARTER, :] = keep[mine_rows, DK:]
        give[2 * QUARTER :, :] = jnp.zeros((DK - 2 * QUARTER, DV), F32)


def coupled(mine, other):
    return pl.pallas_call(
        couple_kernel,
        in_specs=[VMEM] * 2,
        out_specs=[VMEM] * 2,
        out_shape=[jax.ShapeDtypeStruct((DK, DK + DV), F32), jax.ShapeDtypeStruct((DK, DV), F32)],
        compiler_params=granted(4),
    )(mine, other)


def owner_kernel(keep, got, query, state, read):
    place = lax.axis_index("sp")
    late = (place // 2) % 2 == 1
    core = place % 2
    rows = pl.ds(pl.multiple_of(2 * QUARTER + core * QUARTER, QUARTER), QUARTER)
    early = jnp.where(late, got[...], keep[:, DK:])
    last_map = jnp.where(late, keep[rows, :DK], got[0:QUARTER, :])
    last_add = jnp.where(late, keep[rows, DK:], got[QUARTER : 2 * QUARTER, :])
    owned = (dot3(last_map, early) + last_add).astype(BF16)
    state[...] = owned
    which = lax.broadcasted_iota(jnp.int32, query.shape, 0)
    lane = lax.broadcasted_iota(jnp.int32, query.shape, 1)
    chosen = (which == place // 4) & (lane // QUARTER == place % 4)
    picked = jnp.where(chosen, query[...].astype(F32), 0.0).astype(BF16)
    tall = jnp.concatenate([owned] * (DK // QUARTER), axis=0)
    read[...] = jnp.sum(dot1(picked, tall), axis=0, keepdims=True)


def owner_rows(keep, got, query):
    return pl.pallas_call(
        owner_kernel,
        in_specs=[VMEM] * 3,
        out_specs=[VMEM] * 2,
        out_shape=[jax.ShapeDtypeStruct((QUARTER, DV), BF16), jax.ShapeDtypeStruct((1, DV), F32)],
        compiler_params=granted(4),
    )(keep, got, query)


def shards(
    layer_input,
    w_key,
    w_value,
    w_gates,
    decay_rate,
    beta_bias,
    log_decay_extra,
    new_query,
    read_gain,
):
    prompts, _, _ = layer_input.shape
    sp = lax.axis_size("sp")
    tp = lax.axis_size("tp")
    chunks = sp // prompts
    place = lax.axis_index("sp")
    pair = [(i, i ^ 1) for i in range(tp)]
    picked = jnp.where(place % 2 == 1, w_value, w_key)
    first = lax.ppermute(picked, "tp", pair)
    second = lax.ppermute(first, "sp", [(i, i ^ 1) for i in range(sp)])

    sent = packed(layer_input, log_decay_extra[:, 0, :])
    groups = [[prompts * t + j for j in range(prompts)] for t in range(chunks)]
    here = lax.all_to_all(sent, "sp", 0, 0, axis_index_groups=groups, tiled=True)

    parcel = parcels(here, decay_rate, beta_bias, tp)
    gathered = lax.all_to_all(parcel, "tp", 0, 0, tiled=True)

    gate_rows = w_gates.transpose(0, 2, 1).reshape(2 * tp, -1)
    gates = gate_sums(gathered, gate_rows)
    theirs = head_call(partner_kernel, gathered, first, second, gates)
    other = lax.ppermute(theirs, "tp", pair)
    mine = head_call(own_kernel, gathered, w_key, w_value, gates)
    whole = pair_composed(mine, other)

    ways = [
        (prompts * t + i, chunks * ((2 * t + SHIFT + i) % prompts) + t)
        for t in range(chunks)
        for i in range(prompts)
    ]
    moved = lax.ppermute(whole, "sp", ways)
    near = lax.ppermute(moved, "sp", [(i, i ^ 1) for i in range(sp)])
    keep, give = coupled(moved, near)
    got = lax.ppermute(give, "sp", [(i, i ^ 2) for i in range(sp)])
    state_cache, partial = owner_rows(keep, got, new_query)

    parts = lax.all_to_all(
        jnp.broadcast_to(partial[None], (sp, 1, DV)), "sp", 0, 0, tiled=True
    )
    raw = parts.reshape(prompts, chunks, DV).sum(axis=1)
    scaled = raw * lax.rsqrt(jnp.mean(raw * raw, axis=-1, keepdims=True) + EPS) * read_gain
    return state_cache, scaled.astype(BF16)


def solution(mesh):
    placed = (
        P(None, "sp", "tp"),
        P(None, "tp"),
        P(None, "tp"),
        P(),
        P("tp"),
        P("tp"),
        P(None, "tp", "sp"),
        P(None, "tp"),
        P(),
    )

    return jax.shard_map(
        shards, mesh=mesh, in_specs=placed, out_specs=(P("sp", "tp"), P(None, "tp")), check_vma=False
    )
```
